32 devices in a mesh: sp: 8 (over z, y), tp: 4 (over x, core).
Axes of the slice: x: 2, y: 2, z: 4, core: 2. Of those that a mesh axis runs over, the one named last changes fastest.
Arguments:
- residual: bfloat16 [2048, 2048], P(('sp', 'tp')), may hold values from -6 to 6
- ssm_input: bfloat16 [2048, 2048], P('sp', 'tp'), may hold values from -6 to 6
- pole_real: float32 [128, 64], P('tp'), may hold values from -2 to 0
- pole_imaginary: float32 [128, 64], P('tp'), may hold values from 1 to 100
- step_log: float32 [128], P('tp'), may hold values from -8 to 0
- input_real: float32 [128, 64, 16], P('tp'), may hold values from -1 to 1
- entry_map_quadrature: float32 [128, 64, 16], P('tp'), may hold values from -1 to 1
- output_real: float32 [128, 16, 64], P('tp'), may hold values from -0.5 to 0.5
- output_imaginary: float32 [128, 16, 64], P('tp'), may hold values from -0.5 to 0.5
- added_log_decay: float32 [2048, 128], P('sp', 'tp'), may hold values from -2 to 0
- out_weight: bfloat16 [2048, 2048], P('tp'), may hold values from -0.125 to 0.125
- mix_gain: float32 [2048], replicated, may hold values from 0.1 to 1.9
- gate_weight: bfloat16 [2048, 5632], P('sp', 'tp'), may hold values from -0.125 to 0.125
- up_weight: bfloat16 [2048, 5632], P('sp', 'tp'), may hold values from -0.125 to 0.125
- down_weight: bfloat16 [2048, 5632], P('sp', 'tp'), may hold values from -0.078125 to 0.078125
- pre_gain: float32 [2048], replicated, may hold values from 0.1 to 1.9
- post_gain: float32 [2048], replicated, may hold values from 0.1 to 1.9
Outputs:
- merged: bfloat16 [2048, 2048], P(('sp', 'tp'))
The draws below stay inside these ranges and needn't reach their ends.
All inputs are finite; a program needn't handle non-finite values.
Results may differ from the reference program's by a relative error of at most 0.017.
Values may be sent and summed in bfloat16 or wider, within the bound.
A program may use at most 128 MiB of HBM per device.

```python
import math
import jax
import jax.numpy as jnp
from jax import lax

D = 2048
FF = 5632
SSM_WIDTH = 2048
GROUP_CH = 16
STATE = 64
TOK_DEV = 256
CHANNEL_BUNDLES = 128
SEQUENCE_ITEMS = 2048


def frequency_lookup(key):
    base = jax.random.fold_in(key, 11)
    pick_key, slow_key, quick_random_seed, spread_key = jax.random.split(base, 4)
    slow_count = 5
    slow_flag = jax.random.randint(pick_key, (CHANNEL_BUNDLES,), 0, 10) < slow_count
    slow_rate = jnp.exp(jax.random.uniform(slow_key, (CHANNEL_BUNDLES,), jnp.float32, math.log(0.05), math.log(0.5))) / SEQUENCE_ITEMS
    fast_rate = jnp.exp(jax.random.uniform(quick_random_seed, (CHANNEL_BUNDLES,), jnp.float32, math.log(8.0), math.log(16.0))) / TOK_DEV
    rate = jnp.where(slow_flag, slow_rate, fast_rate)
    dispersion = jnp.exp(jax.random.uniform(spread_key, (CHANNEL_BUNDLES, STATE), jnp.float32, -0.3, 0.3))
    return (rate, dispersion)


def draw_pole_real(key, part):
    rate, dispersion = frequency_lookup(key)
    return -jnp.sqrt(rate)[:, None] * dispersion


def draw_step_log(key, part):
    rate, dispersion = frequency_lookup(key)
    return 0.5 * jnp.log(rate)


def draw_added_log_decay(key, part):
    base = jax.random.fold_in(key, 23)
    level_key, where_key, damping_random_seed = jax.random.split(base, 3)
    block_count = SEQUENCE_ITEMS // TOK_DEV
    level = jax.random.uniform(level_key, (block_count, CHANNEL_BUNDLES), jnp.float32, 0.0, 0.4) / SEQUENCE_ITEMS
    baseline_constant = jnp.repeat(level, TOK_DEV, axis=0)
    locations = jax.random.randint(where_key, (2, CHANNEL_BUNDLES), 0, SEQUENCE_ITEMS)
    damping_charges = jax.random.uniform(damping_random_seed, (2, CHANNEL_BUNDLES), jnp.float32, 0.2, 0.4)
    impulse_slots = jnp.arange(SEQUENCE_ITEMS)[:, None, None] == locations[None]
    impulse_tallies = jnp.sum(jnp.where(impulse_slots, jnp.log1p(-damping_charges)[None], 0.0), axis=1)
    return impulse_tallies - baseline_constant


def steps_of(rng, extent, shards, low, high):
    level, own = 1.0, jax.random.fold_in(rng, 6)
    for dim, blocks in shards:
        steps = jnp.exp(jax.random.uniform(jax.random.fold_in(own, dim), (blocks,), jnp.float32, low / len(shards), high / len(shards)))
        level = level * jnp.repeat(steps, extent[dim] // blocks).reshape([-1 if axis == dim else 1 for axis in range(len(extent))])
    return level


def normal_values(own_key, dims, scale, limit, cuts=(), held_as=jnp.bfloat16):
    entries = scale * jax.random.normal(own_key, dims, jnp.float32)
    if cuts:
        entries = entries * steps_of(own_key, dims, cuts, -0.22, 0.18)
    return jnp.clip(entries, -limit, limit).astype(held_as)


def setup_inputs(seed: int = 0) -> dict:
    key_of = jax.random.split(jax.random.key(seed), 18)
    residual = normal_values(key_of[0], (SEQUENCE_ITEMS, D), 1.0, 6.0, ((0, 32),))
    ssm_input = normal_values(key_of[1], (SEQUENCE_ITEMS, SSM_WIDTH), 1.0, 6.0, ((0, 8), (1, 4)))
    pole_real = draw_pole_real(jax.random.fold_in(key_of[17], 71), 0)
    pole_imaginary = jnp.clip(1.0 + 99.0 * jax.random.uniform(key_of[3], (CHANNEL_BUNDLES, STATE), jnp.float32) ** steps_of(key_of[3], (CHANNEL_BUNDLES, STATE), ((0, 4),), -0.2, 0.2), 1.0, 100.0)
    step_log = draw_step_log(jax.random.fold_in(key_of[17], 71), 0)
    input_real = normal_values(key_of[5], (CHANNEL_BUNDLES, STATE, GROUP_CH), (2 * GROUP_CH) ** -0.5, 1.0, ((0, 4),), jnp.float32)
    entry_map_quadrature = normal_values(key_of[6], (CHANNEL_BUNDLES, STATE, GROUP_CH), (2 * GROUP_CH) ** -0.5, 1.0, ((0, 4),), jnp.float32)
    output_real = normal_values(key_of[7], (CHANNEL_BUNDLES, GROUP_CH, STATE), (2 * STATE) ** -0.5, 0.5, ((0, 4),), jnp.float32)
    output_imaginary = normal_values(key_of[8], (CHANNEL_BUNDLES, GROUP_CH, STATE), (2 * STATE) ** -0.5, 0.5, ((0, 4),), jnp.float32)
    added_log_decay = draw_added_log_decay(jax.random.fold_in(key_of[17], 71), 0)
    out_weight = normal_values(key_of[10], (SSM_WIDTH, D), SSM_WIDTH ** -0.5, 0.125, ((0, 4),))
    mix_gain = jnp.clip(1.0 + 0.18 * jax.random.normal(key_of[11], (D,), jnp.float32), 0.1, 1.9)
    gate_weight = normal_values(key_of[12], (D, FF), D ** -0.5, 0.125, ((0, 8), (1, 4)))
    up_weight = normal_values(key_of[13], (D, FF), D ** -0.5, 0.125, ((0, 8), (1, 4)))
    down_weight = normal_values(key_of[14], (D, FF), FF ** -0.5, 0.078125, ((0, 8), (1, 4)))
    pre_gain = jnp.clip(1.0 + 0.18 * jax.random.normal(key_of[15], (D,), jnp.float32), 0.1, 1.9)
    post_gain = jnp.clip(1.0 + 0.18 * jax.random.normal(key_of[16], (D,), jnp.float32), 0.1, 1.9)
    return {"residual": residual, "ssm_input": ssm_input, "pole_real": pole_real, "pole_imaginary": pole_imaginary, "step_log": step_log, "input_real": input_real, "entry_map_quadrature": entry_map_quadrature, "output_real": output_real, "output_imaginary": output_imaginary, "added_log_decay": added_log_decay, "out_weight": out_weight, "mix_gain": mix_gain, "gate_weight": gate_weight, "up_weight": up_weight, "down_weight": down_weight, "pre_gain": pre_gain, "post_gain": post_gain}


EXACT = lax.Precision.HIGHEST
EPSILON = 1e-06

def rms_scale(values, gain):
    return values * lax.rsqrt(lax.optimization_barrier(jnp.mean(values * values, axis=-1, keepdims=True)) + EPSILON) * gain

def round_half(values):
    return lax.optimization_barrier(values.astype(jnp.bfloat16))

def chain_link(earlier, later):
    decay_real, decay_imaginary, state_real, state_imaginary = earlier
    next_real, next_imaginary, drive_real, drive_imaginary = later
    return (next_real * decay_real - next_imaginary * decay_imaginary, next_real * decay_imaginary + next_imaginary * decay_real, next_real * state_real - next_imaginary * state_imaginary + drive_real, next_real * state_imaginary + next_imaginary * state_real + drive_imaginary)

def local_states(inputs, pole_real, pole_imaginary, step_log, input_real, entry_map_quadrature, added_log_decay):
    row_count = inputs.shape[0]
    groups, hidden_states = pole_real.shape
    width = input_real.shape[2]
    step_size = jnp.exp(step_log)[:, None]
    log_size = pole_real * step_size
    angle = pole_imaginary * step_size
    cosine = jnp.cos(angle)
    sine = jnp.sin(angle)
    lift_real = jnp.expm1(log_size) * cosine - 2.0 * jnp.sin(0.5 * angle) ** 2
    lift_imaginary = jnp.exp(log_size) * sine
    denominator = pole_real * pole_real + pole_imaginary * pole_imaginary
    ratio_real = (lift_real * pole_real + lift_imaginary * pole_imaginary) / denominator
    ratio_imaginary = (lift_imaginary * pole_real - lift_real * pole_imaginary) / denominator
    bar_real = ratio_real[..., None] * input_real - ratio_imaginary[..., None] * entry_map_quadrature
    bar_imaginary = ratio_real[..., None] * entry_map_quadrature + ratio_imaginary[..., None] * input_real
    grouped = inputs.astype(jnp.float32).reshape(row_count, groups, width)
    drive_real = jnp.einsum('gnc,tgc->tgn', bar_real, grouped, precision=EXACT).reshape(row_count, groups * hidden_states)
    drive_imaginary = jnp.einsum('gnc,tgc->tgn', bar_imaginary, grouped, precision=EXACT).reshape(row_count, groups * hidden_states)
    pole_magnitude = jnp.exp(log_size[None] + added_log_decay[:, :, None])
    decay_real = (pole_magnitude * cosine[None]).reshape(row_count, groups * hidden_states)
    decay_imaginary = (pole_magnitude * sine[None]).reshape(row_count, groups * hidden_states)
    return lax.associative_scan(chain_link, (decay_real, decay_imaginary, drive_real, drive_imaginary), axis=0)

def apply_carry(scanned, carry_real, carry_imaginary):
    product_real, product_imaginary, state_real, state_imaginary = scanned
    return (state_real + product_real * carry_real - product_imaginary * carry_imaginary, state_imaginary + product_real * carry_imaginary + product_imaginary * carry_real)

def readout(state_real, state_imaginary, output_real, output_imaginary):
    groups, width, hidden_states = output_real.shape
    row_count = state_real.shape[0]
    real_part = jnp.einsum('gcn,tgn->tgc', output_real, state_real.reshape(row_count, groups, hidden_states), precision=EXACT)
    other_part = jnp.einsum('gcn,tgn->tgc', output_imaginary, state_imaginary.reshape(row_count, groups, hidden_states), precision=EXACT)
    return jax.nn.gelu((real_part - other_part).reshape(row_count, groups * width)).astype(jnp.bfloat16)

def reference(residual, ssm_input, pole_real, pole_imaginary, step_log, input_real, entry_map_quadrature, output_real, output_imaginary, added_log_decay, out_weight, mix_gain, gate_weight, up_weight, down_weight, pre_gain, post_gain):
    block_count = SEQUENCE_ITEMS // TOK_DEV

    def per_block(carry, inputs):
        rows_residual, rows_input, rows_extra = inputs
        scanned = local_states(rows_input, pole_real, pole_imaginary, step_log, input_real, entry_map_quadrature, rows_extra)
        state_real, state_imaginary = apply_carry(scanned, carry[0], carry[1])
        activated = readout(state_real, state_imaginary, output_real, output_imaginary)
        mixed = jnp.dot(activated, out_weight, preferred_element_type=jnp.float32)
        middle = round_half(rows_residual.astype(jnp.float32) + rms_scale(mixed, mix_gain))
        mixer_input = rms_scale(middle.astype(jnp.float32), pre_gain).astype(jnp.bfloat16)
        gate_act = jnp.dot(mixer_input, gate_weight, preferred_element_type=jnp.float32)
        up_act = jnp.dot(mixer_input, up_weight, preferred_element_type=jnp.float32)
        hidden = (jax.nn.silu(gate_act) * up_act).astype(jnp.bfloat16)
        mixer_out = lax.dot_general(hidden, down_weight, (((1,), (1,)), ((), ())), preferred_element_type=jnp.float32)
        merged = (middle.astype(jnp.float32) + 0.5 * rms_scale(mixer_out, post_gain)).astype(jnp.bfloat16)
        return ((state_real[-1], state_imaginary[-1]), merged)
    flat_width = pole_real.shape[0] * pole_real.shape[1]
    initial = (jnp.zeros((flat_width,), jnp.float32), jnp.zeros((flat_width,), jnp.float32))
    _, outputs = lax.scan(per_block, initial, (residual.reshape(block_count, TOK_DEV, D), ssm_input.reshape(block_count, TOK_DEV, SSM_WIDTH), added_log_decay.reshape(block_count, TOK_DEV, CHANNEL_BUNDLES)))
    return outputs.reshape(SEQUENCE_ITEMS, D)
```

```python
import functools
import math

import jax
import jax.numpy as jnp
from jax import lax
from jax.experimental import pallas as pl
from jax.experimental.pallas import tpu as pltpu
from jax.sharding import PartitionSpec as P

EPSILON = 1e-06
CHUNKS = 8
LANES = 128
BLOCK = 512
CORES = 2
MESH = pl.DeviceIdType.MESH


def rms_scale(values, gain):
    return values * lax.rsqrt(jnp.mean(values * values, axis=-1, keepdims=True) + EPSILON) * gain


def split(values):
    high = values.astype(jnp.bfloat16)
    return high, (values - high.astype(jnp.float32)).astype(jnp.bfloat16)


def dot32(a, b):
    return jnp.dot(a, b, preferred_element_type=jnp.float32)


def times(ar, ai, br, bi):
    return ar * br - ai * bi, ar * bi + ai * br


class Links:
    def __init__(self, n, nt, nz):
        self.nz, self.ny, self.nx, self.nc = nz, n // nz, nt // CORES, CORES
        sp, tp = lax.axis_index("sp"), lax.axis_index("tp")
        self.z, self.y = lax.div(sp, self.ny), lax.rem(sp, self.ny)
        self.x, self.c = lax.div(tp, self.nc), lax.rem(tp, self.nc)
        self.sent = []

    def far(self, dz=0, dy=0, dx=0, dc=0):
        return {
            "sp": lax.rem(self.z + dz, self.nz) * self.ny + lax.rem(self.y + dy, self.ny),
            "tp": lax.rem(self.x + dx, self.nx) * self.nc + lax.rem(self.c + dc, self.nc),
        }

    def copy(self, src, dst, sems, index, device):
        made = pltpu.make_async_remote_copy(
            src_ref=src,
            dst_ref=dst,
            send_sem=sems.at[(0,) + index],
            recv_sem=sems.at[(1,) + index],
            device_id=device,
            device_id_type=MESH,
        )
        made.start()
        self.sent.append(made)
        return made


def span(index, size):
    return pl.ds(pl.multiple_of(index * size, size), size)


class Weights:
    def __init__(self, links, sources, held, local, z_sem, x_sem, y_sem, d_sem):
        self.links, self.sources, self.held = links, sources, held
        self.local, self.z_sem, self.x_sem, self.y_sem, self.d_sem = (
            local,
            z_sem,
            x_sem,
            y_sem,
            d_sem,
        )
        self.depth, self.units = sources[0].shape
        self.wide = held.shape[2] // links.nx
        self.coming = {}

    def piece(self, z, x):
        links = self.links
        nt = links.nx * links.nc
        tp = x * links.nc + links.c
        which = lax.rem(z + links.nz * nt - tp - 1, links.nz)
        first = jnp.minimum(which * self.wide, self.units - self.wide)
        return which, pl.multiple_of(first, LANES)

    def spot(self, j, dz, dy, slot):
        links = self.links
        origin = lax.rem(links.z - dz + links.nz, links.nz) * links.ny + lax.rem(
            links.y - dy + links.ny, links.ny
        )
        return self.held.at[j, span(origin, self.depth), pl.ds(slot * self.wide, self.wide)]

    def cut(self, j, dz):
        links = self.links
        _, first = self.piece(lax.rem(links.z + dz, links.nz), links.x)
        return self.sources[j].at[:, pl.ds(first, self.wide)]

    def begin(self):
        links = self.links
        self.own = []
        for j in range(len(self.sources)):
            own = pltpu.make_async_copy(self.cut(j, 0), self.spot(j, 0, 0, 0), self.local.at[j])
            own.start()
            self.own.append(own)

    def along_z(self):
        links = self.links
        for j in range(len(self.sources)):
            for dz in range(1, links.nz):
                self.coming["z", j, dz] = links.copy(
                    self.cut(j, dz), self.spot(j, 0, 0, 0), self.z_sem, (j, dz - 1), links.far(dz=dz)
                )

    def arrive(self, *key):
        made = self.coming.pop(key, None)
        if made is not None:
            made.wait_recv()

    def spread(self, j, zr):
        links = self.links
        if zr == 0:
            self.own[j].wait()
        else:
            self.arrive("z", j, zr)
        here = self.spot(j, zr, 0, 0)
        for dx in range(1, links.nx):
            self.coming["x", j, zr, dx] = links.copy(
                here, self.spot(j, zr, 0, dx), self.x_sem, (j, zr, dx - 1), links.far(dx=dx)
            )
        for dy in range(1, links.ny):
            self.coming["y", j, zr, dy] = links.copy(
                here, here, self.y_sem, (j, zr, dy - 1), links.far(dy=dy)
            )

    def relay(self, j, zr):
        links = self.links
        if (j + zr) % 2 == 0:
            for dx in range(1, links.nx):
                self.arrive("x", j, zr, dx)
                here = self.spot(j, zr, 0, dx)
                for dy in range(1, links.ny):
                    self.coming["d", j, zr, dx, dy] = links.copy(
                        here, here, self.d_sem, (j, zr, dx - 1, dy - 1), links.far(dy=dy)
                    )
        else:
            for dy in range(1, links.ny):
                self.arrive("y", j, zr, dy)
                for dx in range(1, links.nx):
                    self.coming["d", j, zr, dx, dy] = links.copy(
                        self.spot(j, zr, dy, 0),
                        self.spot(j, zr, dy, dx),
                        self.d_sem,
                        (j, zr, dx - 1, dy - 1),
                        links.far(dx=dx),
                    )

    def need(self, j, zr):
        for key in [key for key in self.coming if key[1:3] == (j, zr)]:
            self.arrive(*key)


def layer_kernel(
    n,
    nt,
    nz,
    u,
    mag,
    cr,
    ci,
    er,
    ei,
    rr,
    ri,
    order,
    residual,
    weight,
    mix_gain,
    pre_gain,
    post_gain,
    gate_weight,
    up_weight,
    down_weight,
    out,
    dr,
    di,
    ends,
    send,
    recv,
    start,
    active,
    part,
    pair_land,
    half,
    half_land,
    held,
    rows_all,
    hidden,
    other,
    other_land,
    sums,
    sums_send,
    sums_land,
    send_sem,
    recv_sem,
    local_sem,
    z_sem,
    x_sem,
    y_sem,
    d_sem,
    pair_sem,
    half_sem,
    row_sem,
    row_pair_sem,
    other_sem,
    sums_sem,
):
    me = lax.axis_index("sp")
    links = Links(n, nt, nz)
    nx, nc, ny = links.nx, links.nc, links.ny
    rows, flat = dr.shape
    own = rows // nt
    steps = rows // CHUNKS
    packs, width, wide = er.shape
    block = min(BLOCK, flat)

    barrier = pltpu.get_barrier_semaphore()
    for d in range(1, n):
        pl.semaphore_signal(
            barrier, inc=1, device_id={"sp": lax.rem(me + d, n)}, device_id_type=MESH
        )
    place = lax.axis_index("tp")
    for d in range(1, nt):
        pl.semaphore_signal(
            barrier, inc=1, device_id={"tp": lax.rem(place + d, nt)}, device_id_type=MESH
        )
    weights = Weights(
        links, (gate_weight, up_weight, down_weight), held, local_sem, z_sem, x_sem, y_sem, d_sem
    )
    weights.begin()
    pl.semaphore_wait(barrier, n - 1 + nt - 1)
    weights.along_z()
    for j in range(3):
        weights.spread(j, 0)

    for p in range(packs):
        piece = u[:, p * width : (p + 1) * width]
        for e, dst in ((er, dr), (ei, di)):
            high, low = split(e[p])
            dst[:, p * wide : (p + 1) * wide] = dot32(piece, high) + dot32(piece, low)

    for b in range(0, flat, block):
        at = pl.ds(b, block)
        kr = jnp.broadcast_to(cr[0:1, at], (CHUNKS, block))
        ki = jnp.broadcast_to(ci[0:1, at], (CHUNKS, block))

        def first(j, held_values):
            pr, pi, sr, si = held_values
            row = pl.ds(pl.multiple_of(j * CHUNKS, CHUNKS), CHUNKS)
            m = mag[row, at]
            ar, ai = m * kr, m * ki
            pr, pi = times(ar, ai, pr, pi)
            sr, si = times(ar, ai, sr, si)
            return pr, pi, sr + dr[row, at], si + di[row, at]

        zero = jnp.zeros((CHUNKS, block), jnp.float32)
        values = lax.fori_loop(0, steps, first, (zero + 1.0, zero, zero, zero), unroll=2)
        for k in range(4):
            ends[k, :, at] = values[k]

    pr, pi, sr, si = (ends[k, 0:1, :] for k in range(4))
    for c in range(1, CHUNKS):
        ar, ai, br, bi = (ends[k, c : c + 1, :] for k in range(4))
        pr, pi = times(ar, ai, pr, pi)
        sr, si = times(ar, ai, sr, si)
        sr, si = sr + br, si + bi
    for k, item in enumerate((pr, pi, sr, si)):
        send[k : k + 1, :] = item[:, : flat // 2]
        send[4 + k : 5 + k, :] = item[:, flat // 2 :]

    copies = []
    for d in range(1, n):
        copy = pltpu.make_async_remote_copy(
            src_ref=send,
            dst_ref=recv.at[me],
            send_sem=send_sem.at[d - 1],
            recv_sem=recv_sem.at[d - 1],
            device_id={"sp": lax.rem(me + d, n)},
            device_id_type=MESH,
        )
        pl.when(me + d < n)(copy.start)
        copies.append(copy)

    for j in range(3):
        weights.relay(j, 0)
    for zr in range(1, nz):
        weights.spread(0, zr)

    for d, copy in enumerate(copies, 1):
        pl.when(me >= d)(copy.wait_recv)

    sr = jnp.zeros((1, flat), jnp.float32)
    si = sr
    for k in range(n - 1):
        ar, ai, br, bi = (
            jnp.concatenate([recv[k, q : q + 1, :], recv[k, 4 + q : 5 + q, :]], axis=1)
            for q in range(4)
        )
        nr, ni = times(ar, ai, sr, si)
        sr = jnp.where(k < me, nr + br, sr)
        si = jnp.where(k < me, ni + bi, si)
    for c in range(CHUNKS):
        start[0, c : c + 1, :] = sr
        start[1, c : c + 1, :] = si
        ar, ai, br, bi = (ends[k, c : c + 1, :] for k in range(4))
        sr, si = times(ar, ai, sr, si)
        sr, si = sr + br, si + bi

    for b in range(0, flat, block):
        at = pl.ds(b, block)
        kr = jnp.broadcast_to(cr[0:1, at], (CHUNKS, block))
        ki = jnp.broadcast_to(ci[0:1, at], (CHUNKS, block))

        def second(j, held_values):
            row = pl.ds(pl.multiple_of(j * CHUNKS, CHUNKS), CHUNKS)
            m = mag[row, at]
            sr, si = times(m * kr, m * ki, *held_values)
            sr, si = sr + dr[row, at], si + di[row, at]
            dr[row, at] = sr
            di[row, at] = si
            return sr, si

        lax.fori_loop(0, steps, second, (start[0, :, at], start[1, :, at]), unroll=2)

    for p in range(packs):
        total = None
        for state, read in ((dr, rr), (di, ri)):
            high, low = split(state[:, p * wide : (p + 1) * wide])
            top, rest = split(read[p])
            term = dot32(high, top) + dot32(high, rest) + dot32(low, top)
            total = term if total is None else total + term
        active[:, p * width : (p + 1) * width] = jax.nn.gelu(total).astype(jnp.bfloat16)

    active[...] = dot32(order[...], active[...]).astype(jnp.bfloat16)
    columns = weight.shape[1]
    for b in range(0, columns, BLOCK):
        at = pl.ds(b, BLOCK)
        part[:, at] = dot32(active[...], weight[:, at]).astype(jnp.bfloat16)

    def rows_of(x, c):
        return span(x * nc + c, own)

    pairs = []
    for dc in range(1, nc):
        for x in range(nx):
            pairs.append(
                links.copy(
                    part.at[rows_of(x, lax.rem(links.c + dc, nc))],
                    pair_land.at[dc - 1, x],
                    pair_sem,
                    (dc - 1, x),
                    links.far(dc=dc),
                )
            )
    for zr in range(1, nz):
        weights.relay(0, zr)
    for made in pairs:
        made.wait_recv()

    def chip_sum(x):
        value = part[rows_of(x, links.c), :].astype(jnp.float32)
        for dc in range(1, nc):
            value = value + pair_land[dc - 1, x].astype(jnp.float32)
        return value

    halves = []
    for dx in range(1, nx):
        half[dx - 1] = chip_sum(lax.rem(links.x + dx, nx)).astype(jnp.bfloat16)
        halves.append(
            links.copy(half.at[dx - 1], half_land.at[dx - 1], half_sem, (dx - 1,), links.far(dx=dx))
        )
    mixed = chip_sum(links.x)
    for dx, made in enumerate(halves):
        made.wait_recv()
        mixed = mixed + half_land[dx].astype(jnp.float32)
    middle = (residual[...].astype(jnp.float32) + rms_scale(mixed, mix_gain[...])).astype(
        jnp.bfloat16
    )
    line = nz * own
    mine = span(links.z, own)
    rows_all[mine, :] = rms_scale(middle.astype(jnp.float32), pre_gain[...]).astype(jnp.bfloat16)
    along = []
    for dz in range(1, nz):
        along.append(
            links.copy(rows_all.at[mine], rows_all.at[mine], row_sem, (dz - 1,), links.far(dz=dz))
        )
    to_pair = []

    def hand_over(zr):
        index = lax.rem(links.z - zr + nz, nz)
        for dc in range(1, nc):
            to_pair.append(
                links.copy(
                    rows_all.at[span(index, own)],
                    rows_all.at[span(dc * nz + index, own)],
                    row_pair_sem,
                    (zr, dc - 1),
                    links.far(dc=dc),
                )
            )

    hand_over(0)
    for zr in range(1, nz):
        weights.spread(1, zr)
    for zr in range(1, nz):
        weights.relay(1, zr)
    for zr in range(1, nz):
        weights.spread(2, zr)
    for zr in range(1, nz):
        along[zr - 1].wait_recv()
        hand_over(zr)
    for zr in range(1, nz):
        weights.relay(2, zr)
    for made in to_pair:
        made.wait_recv()
    for j in range(2):
        for zr in range(nz):
            weights.need(j, zr)

    valid = []
    for slot in range(nx):
        which, begin = weights.piece(links.z, lax.rem(links.x - slot + nx, nx))
        at = lax.broadcasted_iota(jnp.int32, (1, weights.wide), 1)
        valid.append(jnp.where(begin + at >= which * weights.wide, 1.0, 0.0))
    valid = jnp.concatenate(valid, axis=1)

    def mix(b, carry):
        at = span(b, line)
        gate = dot32(rows_all[at, :], held[0])
        up = dot32(rows_all[at, :], held[1])
        hidden[at, :] = (jax.nn.silu(gate) * up * valid).astype(jnp.bfloat16)
        return carry

    lax.fori_loop(0, nc, mix, 0)

    slab = ny * weights.depth
    others = {}

    def place_of(q):
        return span(lax.rem(links.z - q + nz, nz), slab)

    def project(q):
        weights.need(2, q)
        at = place_of(q)
        value = lax.dot_general(
            hidden[...],
            held[2, at, :],
            (((1,), (1,)), ((), ())),
            preferred_element_type=jnp.float32,
        )
        sums[:, at] = value[:line]
        for dc in range(1, nc):
            other[dc - 1, :, at] = value[dc * line : (dc + 1) * line].astype(jnp.bfloat16)
            others[q, dc] = links.copy(
                other.at[dc - 1, :, at],
                other_land.at[dc - 1, :, at],
                other_sem,
                (q, dc - 1),
                links.far(dc=nc - dc),
            )

    parts = []

    def settle(q):
        at = place_of(q)
        value = sums[:, at]
        for dc in range(1, nc):
            others[q, dc].wait_recv()
            value = value + other_land[dc - 1, :, at].astype(jnp.float32)
        sums[:, at] = value
        sums_send[:, at] = value.astype(jnp.bfloat16)
        for dz in range(1, nz):
            parts.append(
                links.copy(
                    sums_send.at[span(lax.rem(links.z + dz, nz), own), at],
                    sums_land.at[dz - 1, :, at],
                    sums_sem,
                    (q, dz - 1),
                    links.far(dz=dz),
                )
            )

    for q in range(nz):
        project(q)
        if q:
            settle(q - 1)
    settle(nz - 1)
    for made in parts:
        made.wait_recv()
    total = sums[mine, :]
    for dz in range(1, nz):
        total = total + sums_land[dz - 1].astype(jnp.float32)
    out[...] = (middle.astype(jnp.float32) + 0.5 * rms_scale(total, post_gain[...])).astype(
        jnp.bfloat16
    )
    for made in links.sent:
        made.wait_send()
    for d, copy in enumerate(copies, 1):
        pl.when(me + d < n)(copy.wait_send)


def shards(
    n,
    nt,
    residual,
    inputs,
    pole_real,
    pole_imaginary,
    step_log,
    input_real,
    entry_map_quadrature,
    output_real,
    output_imaginary,
    added_log_decay,
    out_weight,
    mix_gain,
    gate_weight,
    up_weight,
    down_weight,
    pre_gain,
    post_gain,
):
    rows, channels = inputs.shape
    columns = out_weight.shape[1]
    groups, states = pole_real.shape
    width = input_real.shape[2]
    flat = groups * states
    step_size = jnp.exp(step_log)[:, None]
    log_size = pole_real * step_size
    angle = pole_imaginary * step_size
    cosine = jnp.cos(angle)
    sine = jnp.sin(angle)
    magnitude = jnp.exp(log_size)
    lift_real = jnp.expm1(log_size) * cosine - 2.0 * jnp.sin(0.5 * angle) ** 2
    lift_imaginary = magnitude * sine
    denominator = pole_real * pole_real + pole_imaginary * pole_imaginary
    ratio_real = (lift_real * pole_real + lift_imaginary * pole_imaginary) / denominator
    ratio_imaginary = (lift_imaginary * pole_real - lift_real * pole_imaginary) / denominator
    bar_real = (
        ratio_real[..., None] * input_real - ratio_imaginary[..., None] * entry_map_quadrature
    )
    bar_imaginary = (
        ratio_real[..., None] * entry_map_quadrature + ratio_imaginary[..., None] * input_real
    )
    pack = LANES // width
    packs = groups // pack
    same = jnp.eye(pack, dtype=jnp.float32)

    def entry(bar):
        bar = bar.reshape(packs, pack, states, width).transpose(0, 1, 3, 2)
        return (bar[:, :, :, None, :] * same[None, :, None, :, None]).reshape(
            packs, pack * width, pack * states
        )

    def read(weight):
        weight = weight.reshape(packs, pack, width, states).transpose(0, 1, 3, 2)
        return (weight[:, :, :, None, :] * same[None, :, None, :, None]).reshape(
            packs, pack * states, pack * width
        )

    def mixed_rows(values):
        return values.reshape(CHUNKS, rows // CHUNKS, -1).transpose(1, 0, 2).reshape(rows, -1)

    spread = jnp.repeat(mixed_rows(jnp.exp(added_log_decay)), states, axis=1)
    vmem = pl.BlockSpec(memory_space=pltpu.VMEM)
    place = jnp.arange(rows)
    order = jax.nn.one_hot(
        place % (rows // CHUNKS) * CHUNKS + place // (rows // CHUNKS), rows, dtype=jnp.bfloat16
    )
    nz = math.gcd(n, nt)
    ny, nx = n // nz, nt // CORES
    own = rows // nt
    line = nz * own
    depth, units = gate_weight.shape
    piece = -(-units // (LANES * nz)) * LANES
    bf, f32 = jnp.bfloat16, jnp.float32
    return pl.pallas_call(
        functools.partial(layer_kernel, n, nt, nz),
        out_shape=jax.ShapeDtypeStruct((own, columns), bf),
        in_specs=[vmem] * 14 + [pl.BlockSpec(memory_space=pl.ANY)] * 3,
        out_specs=vmem,
        scratch_shapes=[
            pltpu.VMEM((rows, flat), f32),
            pltpu.VMEM((rows, flat), f32),
            pltpu.VMEM((4, CHUNKS, flat), f32),
            pltpu.VMEM((8, flat // 2), f32),
            pltpu.VMEM((n, 8, flat // 2), f32),
            pltpu.VMEM((2, CHUNKS, flat), f32),
            pltpu.VMEM((rows, channels), bf),
            pltpu.VMEM((rows, columns), bf),
            pltpu.VMEM((CORES - 1, nx, own, columns), bf),
            pltpu.VMEM((nx - 1, own, columns), bf),
            pltpu.VMEM((nx - 1, own, columns), bf),
            pltpu.VMEM((3, n * depth, nx * piece), bf),
            pltpu.VMEM((CORES * line, columns), bf),
            pltpu.VMEM((CORES * line, nx * piece), bf),
            pltpu.VMEM((CORES - 1, line, columns), bf),
            pltpu.VMEM((CORES - 1, line, columns), bf),
            pltpu.VMEM((line, columns), f32),
            pltpu.VMEM((line, columns), bf),
            pltpu.VMEM((nz - 1, own, columns), bf),
            pltpu.SemaphoreType.DMA((n - 1,)),
            pltpu.SemaphoreType.DMA((n - 1,)),
            pltpu.SemaphoreType.DMA((3,)),
            pltpu.SemaphoreType.DMA((2, 3, nz - 1)),
            pltpu.SemaphoreType.DMA((2, 3, nz, nx - 1)),
            pltpu.SemaphoreType.DMA((2, 3, nz, ny - 1)),
            pltpu.SemaphoreType.DMA((2, 3, nz, nx - 1, ny - 1)),
            pltpu.SemaphoreType.DMA((2, CORES - 1, nx)),
            pltpu.SemaphoreType.DMA((2, nx - 1)),
            pltpu.SemaphoreType.DMA((2, nz - 1)),
            pltpu.SemaphoreType.DMA((2, nz, CORES - 1)),
            pltpu.SemaphoreType.DMA((2, nz, CORES - 1)),
            pltpu.SemaphoreType.DMA((2, nz, nz - 1)),
        ],
        compiler_params=pltpu.CompilerParams(
            collective_id=0, has_side_effects=True, vmem_limit_bytes=60 * 1024 * 1024
        ),
    )(
        mixed_rows(inputs),
        spread,
        (magnitude * cosine).reshape(1, flat),
        (magnitude * sine).reshape(1, flat),
        entry(bar_real),
        entry(bar_imaginary),
        read(output_real),
        read(-output_imaginary),
        order,
        residual,
        out_weight,
        mix_gain.reshape(1, columns),
        pre_gain.reshape(1, columns),
        post_gain.reshape(1, columns),
        gate_weight,
        up_weight,
        down_weight,
    )


def solution(mesh):
    return jax.shard_map(
        functools.partial(shards, mesh.shape["sp"], mesh.shape["tp"]),
        mesh=mesh,
        in_specs=(
            P(("sp", "tp"), None),
            P("sp", "tp"),
            P("tp", None),
            P("tp", None),
            P("tp"),
            P("tp", None, None),
            P("tp", None, None),
            P("tp", None, None),
            P("tp", None, None),
            P("sp", "tp"),
            P("tp", None),
            P(),
            P("sp", "tp"),
            P("sp", "tp"),
            P("sp", "tp"),
            P(),
            P(),
        ),
        out_specs=P(("sp", "tp"), None),
        check_vma=False,
    )
```

```python
import functools
import math

import jax
import jax.numpy as jnp
from jax import lax
from jax.experimental import pallas as pl
from jax.experimental.pallas import tpu as pltpu
from jax.sharding import PartitionSpec as P

EPSILON = 1e-06
CHUNKS = 8
LANES = 128
BLOCK = 512
CORES = 2
MESH = pl.DeviceIdType.MESH


def rms_scale(values, gain):
    return values * lax.rsqrt(jnp.mean(values * values, axis=-1, keepdims=True) + EPSILON) * gain


def split(values):
    high = values.astype(jnp.bfloat16)
    return high, (values - high.astype(jnp.float32)).astype(jnp.bfloat16)


def dot32(a, b):
    return jnp.dot(a, b, preferred_element_type=jnp.float32)


def times(ar, ai, br, bi):
    return ar * br - ai * bi, ar * bi + ai * br


def flip(index, mask):
    out, bit = index, 1
    while bit <= mask:
        if mask & bit:
            out = out + bit - 2 * bit * lax.rem(lax.div(index, bit), 2)
        bit *= 2
    return out


def mirror(place, size):
    out = 0
    while size > 1:
        out, place, size = 2 * out + place % 2, place // 2, size // 2
    return out


def across(a, b):
    return lax.dot_general(
        a, b, (((1,), (1,)), ((), ())), preferred_element_type=jnp.float32
    )


def one_hot(where):
    return jnp.where(where, 1.0, 0.0).astype(jnp.bfloat16)


class Links:
    def __init__(self, n, nt, nz):
        self.nz, self.ny, self.nx, self.nc = nz, n // nz, nt // CORES, CORES
        sp, tp = lax.axis_index("sp"), lax.axis_index("tp")
        self.z, self.y = lax.div(sp, self.ny), lax.rem(sp, self.ny)
        self.x, self.c = lax.div(tp, self.nc), lax.rem(tp, self.nc)
        self.sent = []

    def far(self, dz=0, dy=0, dx=0, dc=0):
        return {
            "sp": flip(self.z, dz) * self.ny + lax.rem(self.y + dy, self.ny),
            "tp": lax.rem(self.x + dx, self.nx) * self.nc + lax.rem(self.c + dc, self.nc),
        }

    def copy(self, src, dst, sems, index, device, when=None):
        made = pltpu.make_async_remote_copy(
            src_ref=src,
            dst_ref=dst,
            send_sem=sems.at[(0,) + index],
            recv_sem=sems.at[(1,) + index],
            device_id=device,
            device_id_type=MESH,
        )
        if when is None:
            made.start()
            self.sent.append(made.wait_send)
        else:
            pl.when(when)(made.start)
            self.sent.append(lambda: pl.when(when)(made.wait_send))
        return made


def span(index, size):
    return pl.ds(pl.multiple_of(index * size, size), size)


class Weights:
    def __init__(self, links, sources, held, local, z_sem, x_sem, y_sem, d_sem):
        self.links, self.sources, self.held = links, sources, held
        self.local, self.z_sem, self.x_sem, self.y_sem, self.d_sem = (
            local,
            z_sem,
            x_sem,
            y_sem,
            d_sem,
        )
        self.depth, self.units = sources[0].shape
        self.wide = held.shape[2] // links.nx
        self.thin = self.units - (links.nz - 1) * self.wide
        self.coming = {}

    def piece(self, z, x):
        links = self.links
        nt = links.nx * links.nc
        tp = x * links.nc + links.c
        return lax.rem(z + links.nz * nt - tp - 1, links.nz)

    def last(self, slot):
        links = self.links
        return self.piece(links.z, lax.rem(links.x - slot + links.nx, links.nx)) == links.nz - 1

    def widths(self, last):
        if self.thin == self.wide:
            return ((None, self.wide),)
        return ((jnp.logical_not(last), self.wide), (last, self.thin))

    def spot(self, j, zr, dy, slot, width):
        links = self.links
        origin = flip(links.z, zr) * links.ny + lax.rem(links.y - dy + links.ny, links.ny)
        return self.held.at[j, span(origin, self.depth), pl.ds(slot * self.wide, width)]

    def cut(self, j, which, width):
        first = jnp.minimum(which * self.wide, self.units - width)
        return self.sources[j].at[:, pl.ds(pl.multiple_of(first, LANES), width)]

    def begin(self):
        links = self.links
        which = self.piece(links.z, links.x)
        self.own = []
        for j in range(len(self.sources)):
            for when, width in self.widths(which == links.nz - 1):
                own = pltpu.make_async_copy(
                    self.cut(j, which, width), self.spot(j, 0, 0, 0, width), self.local.at[j]
                )
                if when is None:
                    own.start()
                else:
                    pl.when(when)(own.start)
                self.own.append((j, when, own.wait))

    def clear(self):
        if self.thin < self.wide:
            for slot in range(self.links.nx):

                @pl.when(self.last(slot))
                def _():
                    at = pl.ds(slot * self.wide + self.thin, self.wide - self.thin)
                    self.held[2, :, at] = jnp.zeros(
                        (self.held.shape[1], self.wide - self.thin), self.held.dtype
                    )

    def pass_on(self, key, j, source, target, sems, index, device, last):
        for when, width in self.widths(last):
            made = self.links.copy(source(width), target(width), sems, index, device, when)
            self.coming.setdefault(key, []).append(made)

    def along_z(self, j, zr):
        links = self.links
        which = self.piece(flip(links.z, zr), links.x)
        self.pass_on(
            ("z", j, zr),
            j,
            lambda width: self.cut(j, which, width),
            lambda width: self.spot(j, 0, 0, 0, width),
            self.z_sem,
            (j, zr - 1),
            links.far(dz=zr),
            which == links.nz - 1,
        )

    def arrive(self, *key):
        slot = {"z": 0, "y": 0, "x": key[-1], "d": key[3] if len(key) > 4 else 0}[key[0]]
        made = self.coming.pop(key, None)
        if made is not None:
            for one, (when, _) in zip(made, self.widths(self.last(slot))):
                if when is None:
                    one.wait_recv()
                else:
                    pl.when(when)(one.wait_recv)

    def spread(self, j, zr):
        links = self.links
        if zr == 0:
            for at, when, wait in self.own:
                if at == j:
                    wait() if when is None else pl.when(when)(wait)
        else:
            self.arrive("z", j, zr)
        last = self.last(0)
        for dx in range(1, links.nx):
            self.pass_on(
                ("x", j, zr, dx),
                j,
                lambda width: self.spot(j, zr, 0, 0, width),
                lambda width: self.spot(j, zr, 0, dx, width),
                self.x_sem,
                (j, zr, dx - 1),
                links.far(dx=dx),
                last,
            )
        for dy in range(1, links.ny):
            self.pass_on(
                ("y", j, zr, dy),
                j,
                lambda width: self.spot(j, zr, 0, 0, width),
                lambda width: self.spot(j, zr, 0, 0, width),
                self.y_sem,
                (j, zr, dy - 1),
                links.far(dy=dy),
                last,
            )

    def relay(self, j, zr):
        links = self.links
        over_y = (j + zr) % 2 == 0
        for dx in range(1, links.nx):
            if over_y:
                self.arrive("x", j, zr, dx)
            for dy in range(1, links.ny):
                if not over_y:
                    self.arrive("y", j, zr, dy)
                slot, shift = (dx, 0) if over_y else (0, dy)
                self.pass_on(
                    ("d", j, zr, dx, dy),
                    j,
                    lambda width: self.spot(j, zr, shift, slot, width),
                    lambda width: self.spot(j, zr, shift, dx, width),
                    self.d_sem,
                    (j, zr, dx - 1, dy - 1),
                    links.far(dy=dy) if over_y else links.far(dx=dx),
                    self.last(slot),
                )

    def need(self, j, zr):
        for key in [key for key in self.coming if key[1:3] == (j, zr)]:
            self.arrive(*key)


def layer_kernel(
    n,
    nt,
    nz,
    u,
    added,
    lines,
    entry,
    read,
    residual,
    weight,
    mix_gain,
    pre_gain,
    post_gain,
    gate_weight,
    up_weight,
    down_weight,
    out,
    mag,
    dr,
    di,
    ends,
    send,
    recv,
    start,
    active,
    part,
    pair_land,
    half,
    half_land,
    held,
    rows_all,
    hidden,
    other,
    other_land,
    sums,
    sums_send,
    sums_land,
    send_sem,
    recv_sem,
    local_sem,
    z_sem,
    x_sem,
    y_sem,
    d_sem,
    pair_sem,
    half_sem,
    row_sem,
    row_pair_sem,
    other_sem,
    sums_sem,
):
    me = lax.axis_index("sp")
    links = Links(n, nt, nz)
    nx, nc, ny = links.nx, links.nc, links.ny
    rows, flat = dr.shape
    own = rows // nt
    steps = rows // CHUNKS
    states, width = flat // added.shape[1], entry.shape[1]
    pack = LANES // width
    packs, wide = added.shape[1] // pack, pack * states
    block = min(BLOCK, flat)

    barrier = pltpu.get_barrier_semaphore()
    for d in range(1, n):
        pl.semaphore_signal(
            barrier, inc=1, device_id={"sp": lax.rem(me + d, n)}, device_id_type=MESH
        )
    place = lax.axis_index("tp")
    for d in range(1, nt):
        pl.semaphore_signal(
            barrier, inc=1, device_id={"tp": lax.rem(place + d, nt)}, device_id_type=MESH
        )
    weights = Weights(
        links, (gate_weight, up_weight, down_weight), held, local_sem, z_sem, x_sem, y_sem, d_sem
    )
    weights.begin()
    pl.semaphore_wait(barrier, n - 1 + nt - 1)
    for j in range(2):
        for zr in range(1, nz):
            weights.along_z(j, zr)
    for j in range(3):
        weights.spread(j, 0)
    weights.clear()

    down = lax.broadcasted_iota(jnp.int32, (rows, rows), 0)
    over = lax.broadcasted_iota(jnp.int32, (rows, rows), 1)
    mixing = one_hot(over == lax.rem(down, CHUNKS) * steps + lax.div(down, CHUNKS))
    order = one_hot(over == lax.rem(down, steps) * CHUNKS + lax.div(down, steps))
    mixed_u = dot32(mixing, u[...]).astype(jnp.bfloat16)
    groups = added.shape[1]
    repeat = one_hot(
        lax.div(lax.broadcasted_iota(jnp.int32, (groups, flat), 1), states)
        == lax.broadcasted_iota(jnp.int32, (groups, flat), 0)
    )
    rest = jnp.exp(added[...])
    total = None
    for _ in range(3):
        term = rest.astype(jnp.bfloat16)
        rest = rest - term.astype(jnp.float32)
        term = dot32(dot32(mixing, term).astype(jnp.bfloat16), repeat)
        total = term if total is None else total + term
    mag[...] = total
    same = lax.div(
        lax.broadcasted_iota(jnp.int32, (LANES, wide), 0), width
    ) == lax.div(lax.broadcasted_iota(jnp.int32, (LANES, wide), 1), states)

    def blocks(rows_of_channels):
        return jnp.where(same, jnp.concatenate([rows_of_channels] * pack, axis=0), 0.0)

    cr, ci = lines.at[0:1], lines.at[1:2]
    for p in range(packs):
        at = pl.ds(p * wide, wide)
        piece = mixed_u[:, p * LANES : (p + 1) * LANES]
        ratio = times(lines[2:3, at], lines[3:4, at], entry[0, :, at], entry[1, :, at])
        for bar, dst in zip(ratio, (dr, di)):
            high, low = split(blocks(bar))
            dst[:, at] = dot32(piece, high) + dot32(piece, low)

    for b in range(0, flat, block):
        at = pl.ds(b, block)
        kr = jnp.broadcast_to(cr[0:1, at], (CHUNKS, block))
        ki = jnp.broadcast_to(ci[0:1, at], (CHUNKS, block))

        def first(j, held_values):
            pr, pi, sr, si = held_values
            row = pl.ds(pl.multiple_of(j * CHUNKS, CHUNKS), CHUNKS)
            m = mag[row, at]
            ar, ai = m * kr, m * ki
            pr, pi = times(ar, ai, pr, pi)
            sr, si = times(ar, ai, sr, si)
            return pr, pi, sr + dr[row, at], si + di[row, at]

        zero = jnp.zeros((CHUNKS, block), jnp.float32)
        values = lax.fori_loop(0, steps, first, (zero + 1.0, zero, zero, zero), unroll=2)
        for k in range(4):
            ends[k, :, at] = values[k]

    pr, pi, sr, si = (ends[k, 0:1, :] for k in range(4))
    for c in range(1, CHUNKS):
        ar, ai, br, bi = (ends[k, c : c + 1, :] for k in range(4))
        pr, pi = times(ar, ai, pr, pi)
        sr, si = times(ar, ai, sr, si)
        sr, si = sr + br, si + bi
    for k, item in enumerate((pr, pi, sr, si)):
        send[k : k + 1, :] = item[:, : flat // 2]
        send[4 + k : 5 + k, :] = item[:, flat // 2 :]

    copies = []
    for d in range(1, n):
        copy = pltpu.make_async_remote_copy(
            src_ref=send,
            dst_ref=recv.at[me],
            send_sem=send_sem.at[d - 1],
            recv_sem=recv_sem.at[d - 1],
            device_id={"sp": lax.rem(me + d, n)},
            device_id_type=MESH,
        )
        pl.when(me + d < n)(copy.start)
        copies.append(copy)

    weights.relay(0, 0)
    for d, copy in enumerate(copies, 1):
        pl.when(me >= d)(copy.wait_recv)

    sr = jnp.zeros((1, flat), jnp.float32)
    si = sr
    for k in range(n - 1):
        ar, ai, br, bi = (
            jnp.concatenate([recv[k, q : q + 1, :], recv[k, 4 + q : 5 + q, :]], axis=1)
            for q in range(4)
        )
        nr, ni = times(ar, ai, sr, si)
        sr = jnp.where(k < me, nr + br, sr)
        si = jnp.where(k < me, ni + bi, si)
    for c in range(CHUNKS):
        start[0, c : c + 1, :] = sr
        start[1, c : c + 1, :] = si
        ar, ai, br, bi = (ends[k, c : c + 1, :] for k in range(4))
        sr, si = times(ar, ai, sr, si)
        sr, si = sr + br, si + bi

    for b in range(0, flat, block):
        at = pl.ds(b, block)
        kr = jnp.broadcast_to(cr[0:1, at], (CHUNKS, block))
        ki = jnp.broadcast_to(ci[0:1, at], (CHUNKS, block))

        def second(j, held_values):
            row = pl.ds(pl.multiple_of(j * CHUNKS, CHUNKS), CHUNKS)
            m = mag[row, at]
            sr, si = times(m * kr, m * ki, *held_values)
            sr, si = sr + dr[row, at], si + di[row, at]
            dr[row, at] = sr
            di[row, at] = si
            return sr, si

        lax.fori_loop(0, steps, second, (start[0, :, at], start[1, :, at]), unroll=2)

    for p in range(packs):
        total = None
        at = pl.ds(p * wide, wide)
        for state, part_read in ((dr, read[0, :, at]), (di, -read[1, :, at])):
            high, low = split(state[:, at])
            top, rest = split(blocks(part_read))
            term = across(high, top) + across(high, rest) + across(low, top)
            total = term if total is None else total + term
        active[:, p * LANES : (p + 1) * LANES] = jax.nn.gelu(total).astype(jnp.bfloat16)

    active[...] = dot32(order, active[...]).astype(jnp.bfloat16)
    columns = weight.shape[1]
    for b in range(0, columns, BLOCK):
        at = pl.ds(b, BLOCK)
        part[:, at] = dot32(active[...], weight[:, at]).astype(jnp.bfloat16)

    def rows_of(x, c):
        return span(x * nc + c, own)

    pairs = []
    for dc in range(1, nc):
        for x in range(nx):
            pairs.append(
                links.copy(
                    part.at[rows_of(x, lax.rem(links.c + dc, nc))],
                    pair_land.at[dc - 1, x],
                    pair_sem,
                    (dc - 1, x),
                    links.far(dc=dc),
                )
            )
    weights.relay(1, 0)
    weights.relay(2, 0)
    for zr in range(1, nz):
        weights.spread(0, zr)
    for made in pairs:
        made.wait_recv()

    def chip_sum(x):
        value = part[rows_of(x, links.c), :].astype(jnp.float32)
        for dc in range(1, nc):
            value = value + pair_land[dc - 1, x].astype(jnp.float32)
        return value

    halves = []
    for dx in range(1, nx):
        half[dx - 1] = chip_sum(lax.rem(links.x + dx, nx)).astype(jnp.bfloat16)
        halves.append(
            links.copy(half.at[dx - 1], half_land.at[dx - 1], half_sem, (dx - 1,), links.far(dx=dx))
        )
    mixed = chip_sum(links.x)
    for dx, made in enumerate(halves):
        made.wait_recv()
        mixed = mixed + half_land[dx].astype(jnp.float32)
    middle = (residual[...].astype(jnp.float32) + rms_scale(mixed, mix_gain[...])).astype(
        jnp.bfloat16
    )
    line = nz * own
    bits = [1 << k for k in range(nz.bit_length() - 1)]
    rows_all[:own] = rms_scale(middle.astype(jnp.float32), pre_gain[...]).astype(jnp.bfloat16)
    along = {}
    to_pair = []

    def row_block(zr, dc=0):
        return pl.ds(dc * line + mirror(zr, nz) * own, own)

    def hand_on(zr):
        if zr:
            along[zr].wait_recv()
        for bit in reversed(bits):
            if zr == 0 or bit < (zr & -zr):
                along[zr ^ bit] = links.copy(
                    rows_all.at[row_block(zr)],
                    rows_all.at[row_block(zr ^ bit)],
                    row_sem,
                    ((zr ^ bit) - 1,),
                    links.far(dz=bit),
                )
        for dc in range(1, nc):
            to_pair.append(
                links.copy(
                    rows_all.at[row_block(zr)],
                    rows_all.at[row_block(zr, dc)],
                    row_pair_sem,
                    (zr, dc - 1),
                    links.far(dc=dc),
                )
            )

    hand_on(0)
    for zr in range(1, nz):
        weights.along_z(2, zr)
    for zr in range(1, nz):
        weights.relay(0, zr)
    for zr in range(1, nz):
        weights.spread(1, zr)
    for zr in sorted(range(1, nz), key=lambda zr: -(zr & -zr)):
        hand_on(zr)
    for zr in range(1, nz):
        weights.relay(1, zr)
    for zr in range(1, nz):
        weights.spread(2, zr)
    for made in to_pair:
        made.wait_recv()
    for j in range(2):
        for zr in range(nz):
            weights.need(j, zr)

    valid = []
    for slot in range(nx):
        at = lax.broadcasted_iota(jnp.int32, (1, weights.wide), 1)
        limit = jnp.where(weights.last(slot), weights.thin, weights.wide)
        valid.append(jnp.where(at < limit, 1.0, 0.0))
    valid = jnp.concatenate(valid, axis=1)

    def mix(b, carry):
        at = span(b, line)
        gate = dot32(rows_all[at, :], held[0])
        up = dot32(rows_all[at, :], held[1])
        hidden[at, :] = jnp.where(valid > 0.0, jax.nn.silu(gate) * up, 0.0).astype(jnp.bfloat16)
        return carry

    lax.fori_loop(0, nc, mix, 0)
    for zr in range(1, nz):
        weights.relay(2, zr)

    slab = ny * weights.depth
    others = {}
    parts = {}

    def place_of(q):
        return span(flip(links.z, q), slab)

    def project(q):
        weights.need(2, q)
        at = place_of(q)
        value = across(hidden[...], held[2, at, :])
        sums[:, at] = value[:line]
        for dc in range(1, nc):
            other[dc - 1, :, at] = value[dc * line : (dc + 1) * line].astype(jnp.bfloat16)
            others[q, dc] = links.copy(
                other.at[dc - 1, :, at],
                other_land.at[dc - 1, :, at],
                other_sem,
                (q, dc - 1),
                links.far(dc=nc - dc),
            )

    def give(q, level, value):
        if level == len(bits):
            sums[:own, place_of(q)] = value
            return
        at = place_of(q)
        count = value.shape[0] // 2
        half_rows = pl.ds(count, count)
        sums[:count, at] = value[:count]
        sums_send[half_rows, at] = value[count:].astype(jnp.bfloat16)
        parts[q ^ bits[level], level] = links.copy(
            sums_send.at[half_rows, at],
            sums_land.at[half_rows, at],
            sums_sem,
            (q ^ bits[level], level),
            links.far(dz=bits[level]),
        )

    def take(q, level):
        at = place_of(q)
        count = line >> (level + 1)
        parts[q, level].wait_recv()
        land = sums_land[pl.ds(count, count), at].astype(jnp.float32)
        give(q, level + 1, sums[:count, at] + land)

    def settle(q):
        at = place_of(q)
        value = sums[:, at]
        for dc in range(1, nc):
            others[q, dc].wait_recv()
            value = value + other_land[dc - 1, :, at].astype(jnp.float32)
        give(q, 0, value)

    taken = 0
    for q in range(nz):
        project(q)
        if q % 2 or q == nz - 1:
            for done in range(q - q % 2, q + 1):
                settle(done)
            while bits and taken < q - 1:
                take(taken, 0)
                taken += 1
    for q in range(taken if bits else nz, nz):
        take(q, 0)
    for level in range(1, len(bits)):
        for q in range(nz):
            take(q, level)
    total = sums[:own, :]
    out[...] = (middle.astype(jnp.float32) + 0.5 * rms_scale(total, post_gain[...])).astype(
        jnp.bfloat16
    )
    for wait in links.sent:
        wait()
    for d, copy in enumerate(copies, 1):
        pl.when(me + d < n)(copy.wait_send)


def shards(
    n,
    nt,
    residual,
    inputs,
    pole_real,
    pole_imaginary,
    step_log,
    input_real,
    entry_map_quadrature,
    output_real,
    output_imaginary,
    added_log_decay,
    out_weight,
    mix_gain,
    gate_weight,
    up_weight,
    down_weight,
    pre_gain,
    post_gain,
):
    rows, channels = inputs.shape
    columns = out_weight.shape[1]
    groups, states = pole_real.shape
    width = input_real.shape[2]
    flat = groups * states
    step_size = jnp.exp(step_log)[:, None]
    log_size = pole_real * step_size
    angle = pole_imaginary * step_size
    cosine = jnp.cos(angle)
    sine = jnp.sin(angle)
    magnitude = jnp.exp(log_size)
    lift_real = jnp.expm1(log_size) * cosine - 2.0 * jnp.sin(0.5 * angle) ** 2
    lift_imaginary = magnitude * sine
    denominator = pole_real * pole_real + pole_imaginary * pole_imaginary
    ratio_real = (lift_real * pole_real + lift_imaginary * pole_imaginary) / denominator
    ratio_imaginary = (lift_imaginary * pole_real - lift_real * pole_imaginary) / denominator
    lines = jnp.stack(
        (magnitude * cosine, magnitude * sine, ratio_real, ratio_imaginary)
    ).reshape(4, flat)
    entry = jnp.stack((input_real, entry_map_quadrature)).transpose(0, 3, 1, 2)
    read = jnp.stack((output_real, output_imaginary)).transpose(0, 2, 1, 3)
    vmem = pl.BlockSpec(memory_space=pltpu.VMEM)
    nz = math.gcd(n, nt)
    nz = nz & -nz
    ny, nx = n // nz, nt // CORES
    own = rows // nt
    line = nz * own
    depth, units = gate_weight.shape
    piece = -(-units // (LANES * nz)) * LANES
    bf, f32 = jnp.bfloat16, jnp.float32
    return pl.pallas_call(
        functools.partial(layer_kernel, n, nt, nz),
        out_shape=jax.ShapeDtypeStruct((own, columns), bf),
        in_specs=[vmem] * 10 + [pl.BlockSpec(memory_space=pl.ANY)] * 3,
        out_specs=vmem,
        scratch_shapes=[
            pltpu.VMEM((rows, flat), f32),
            pltpu.VMEM((rows, flat), f32),
            pltpu.VMEM((rows, flat), f32),
            pltpu.VMEM((4, CHUNKS, flat), f32),
            pltpu.VMEM((8, flat // 2), f32),
            pltpu.VMEM((n, 8, flat // 2), f32),
            pltpu.VMEM((2, CHUNKS, flat), f32),
            pltpu.VMEM((rows, channels), bf),
            pltpu.VMEM((rows, columns), bf),
            pltpu.VMEM((CORES - 1, nx, own, columns), bf),
            pltpu.VMEM((nx - 1, own, columns), bf),
            pltpu.VMEM((nx - 1, own, columns), bf),
            pltpu.VMEM((3, n * depth, nx * piece), bf),
            pltpu.VMEM((CORES * line, columns), bf),
            pltpu.VMEM((CORES * line, nx * piece), bf),
            pltpu.VMEM((CORES - 1, line, columns), bf),
            pltpu.VMEM((CORES - 1, line, columns), bf),
            pltpu.VMEM((line, columns), f32),
            pltpu.VMEM((line, columns), bf),
            pltpu.VMEM((line, columns), bf),
            pltpu.SemaphoreType.DMA((n - 1,)),
            pltpu.SemaphoreType.DMA((n - 1,)),
            pltpu.SemaphoreType.DMA((3,)),
            pltpu.SemaphoreType.DMA((2, 3, nz - 1)),
            pltpu.SemaphoreType.DMA((2, 3, nz, nx - 1)),
            pltpu.SemaphoreType.DMA((2, 3, nz, ny - 1)),
            pltpu.SemaphoreType.DMA((2, 3, nz, nx - 1, ny - 1)),
            pltpu.SemaphoreType.DMA((2, CORES - 1, nx)),
            pltpu.SemaphoreType.DMA((2, nx - 1)),
            pltpu.SemaphoreType.DMA((2, nz - 1)),
            pltpu.SemaphoreType.DMA((2, nz, CORES - 1)),
            pltpu.SemaphoreType.DMA((2, nz, CORES - 1)),
            pltpu.SemaphoreType.DMA((2, nz, nz.bit_length())),
        ],
        compiler_params=pltpu.CompilerParams(
            collective_id=0, has_side_effects=True, vmem_limit_bytes=60 * 1024 * 1024
        ),
    )(
        inputs,
        added_log_decay,
        lines,
        entry.reshape(2, width, flat),
        read.reshape(2, width, flat),
        residual,
        out_weight,
        mix_gain.reshape(1, columns),
        pre_gain.reshape(1, columns),
        post_gain.reshape(1, columns),
        gate_weight,
        up_weight,
        down_weight,
    )


def solution(mesh):
    return jax.shard_map(
        functools.partial(shards, mesh.shape["sp"], mesh.shape["tp"]),
        mesh=mesh,
        in_specs=(
            P(("sp", "tp"), None),
            P("sp", "tp"),
            P("tp", None),
            P("tp", None),
            P("tp"),
            P("tp", None, None),
            P("tp", None, None),
            P("tp", None, None),
            P("tp", None, None),
            P("sp", "tp"),
            P("tp", None),
            P(),
            P("sp", "tp"),
            P("sp", "tp"),
            P("sp", "tp"),
            P(),
            P(),
        ),
        out_specs=P(("sp", "tp"), None),
        check_vma=False,
    )
```

```python
import functools
import math

import jax
import jax.numpy as jnp
from jax import lax
from jax.experimental import pallas as pl
from jax.experimental.pallas import tpu as pltpu
from jax.sharding import PartitionSpec as P

EPSILON = 1e-06
CHUNKS = 8
LANES = 128
BLOCK = 512
CORES = 2
MESH = pl.DeviceIdType.MESH


def rms_scale(values, gain):
    return values * lax.rsqrt(jnp.mean(values * values, axis=-1, keepdims=True) + EPSILON) * gain


def split(values):
    high = values.astype(jnp.bfloat16)
    return high, (values - high.astype(jnp.float32)).astype(jnp.bfloat16)


def dot32(a, b):
    return jnp.dot(a, b, preferred_element_type=jnp.float32)


def times(ar, ai, br, bi):
    return ar * br - ai * bi, ar * bi + ai * br


def flip(index, mask):
    out, bit = index, 1
    while bit <= mask:
        if mask & bit:
            out = out + bit - 2 * bit * lax.rem(lax.div(index, bit), 2)
        bit *= 2
    return out


def mirror(place, size):
    out = 0
    while size > 1:
        out, place, size = 2 * out + place % 2, place // 2, size // 2
    return out


def across(a, b):
    return lax.dot_general(
        a, b, (((1,), (1,)), ((), ())), preferred_element_type=jnp.float32
    )


def one_hot(where):
    return jnp.where(where, 1.0, 0.0).astype(jnp.bfloat16)


class Links:
    def __init__(self, n, nt, nz):
        self.nz, self.ny, self.nx, self.nc = nz, n // nz, nt // CORES, CORES
        sp, tp = lax.axis_index("sp"), lax.axis_index("tp")
        self.z, self.y = lax.div(sp, self.ny), lax.rem(sp, self.ny)
        self.x, self.c = lax.div(tp, self.nc), lax.rem(tp, self.nc)
        self.sent = []

    def far(self, dz=0, dy=0, dx=0, dc=0):
        return {
            "sp": flip(self.z, dz) * self.ny + lax.rem(self.y + dy, self.ny),
            "tp": lax.rem(self.x + dx, self.nx) * self.nc + lax.rem(self.c + dc, self.nc),
        }

    def copy(self, src, dst, sems, index, device, when=None):
        made = pltpu.make_async_remote_copy(
            src_ref=src,
            dst_ref=dst,
            send_sem=sems.at[(0,) + index],
            recv_sem=sems.at[(1,) + index],
            device_id=device,
            device_id_type=MESH,
        )
        if when is None:
            made.start()
            self.sent.append(made.wait_send)
        else:
            pl.when(when)(made.start)
            self.sent.append(lambda: pl.when(when)(made.wait_send))
        return made


def span(index, size):
    return pl.ds(pl.multiple_of(index * size, size), size)


class Weights:
    def __init__(self, links, sources, staged, held, local, z_sem, x_sem, y_sem, d_sem):
        self.links, self.sources, self.staged, self.held = links, sources, staged, held
        self.local, self.z_sem, self.x_sem, self.y_sem, self.d_sem = (
            local,
            z_sem,
            x_sem,
            y_sem,
            d_sem,
        )
        self.depth, self.units = sources[0].shape
        self.wide = held.shape[2] // links.nx
        self.thin = self.units - (links.nz - 1) * self.wide
        self.coming = {}

    def piece(self, z, x):
        links = self.links
        nt = links.nx * links.nc
        tp = x * links.nc + links.c
        return lax.rem(z + links.nz * nt - tp - 1, links.nz)

    def last(self, slot):
        links = self.links
        return self.piece(links.z, lax.rem(links.x - slot + links.nx, links.nx)) == links.nz - 1

    def widths(self, last):
        if self.thin == self.wide:
            return ((None, self.wide),)
        return ((jnp.logical_not(last), self.wide), (last, self.thin))

    def spot(self, j, zr, dy, slot, width):
        links = self.links
        origin = flip(links.z, zr) * links.ny + lax.rem(links.y - dy + links.ny, links.ny)
        return self.held.at[j, span(origin, self.depth), pl.ds(slot * self.wide, width)]

    def cut(self, source, which, width):
        first = jnp.minimum(which * self.wide, self.units - width)
        return source.at[:, pl.ds(pl.multiple_of(first, LANES), width)]

    def begin(self):
        links = self.links
        which = self.piece(links.z, links.x)
        self.own = []
        self.whole = [
            pltpu.make_async_copy(source, self.staged.at[j], self.local.at[1, j])
            for j, source in enumerate(self.sources)
        ]
        for j in range(len(self.sources)):
            self.whole[j].start()
            for when, width in self.widths(which == links.nz - 1):
                own = pltpu.make_async_copy(
                    self.cut(self.sources[j], which, width),
                    self.spot(j, 0, 0, 0, width),
                    self.local.at[0, j],
                )
                if when is None:
                    own.start()
                else:
                    pl.when(when)(own.start)
                self.own.append((j, when, own.wait))

    def clear(self):
        if self.thin < self.wide:
            for slot in range(self.links.nx):

                @pl.when(self.last(slot))
                def _():
                    at = pl.ds(slot * self.wide + self.thin, self.wide - self.thin)
                    self.held[2, :, at] = jnp.zeros(
                        (self.held.shape[1], self.wide - self.thin), self.held.dtype
                    )

    def pass_on(self, key, j, source, target, sems, index, device, last):
        for when, width in self.widths(last):
            made = self.links.copy(source(width), target(width), sems, index, device, when)
            self.coming.setdefault(key, []).append(made)

    def along_z(self, j, zr):
        links = self.links
        which = self.piece(flip(links.z, zr), links.x)
        if zr == 1:
            self.whole[j].wait()
        self.pass_on(
            ("z", j, zr),
            j,
            lambda width: self.cut(self.staged.at[j], which, width),
            lambda width: self.spot(j, 0, 0, 0, width),
            self.z_sem,
            (j, zr - 1),
            links.far(dz=zr),
            which == links.nz - 1,
        )

    def arrive(self, *key):
        slot = {"z": 0, "y": 0, "x": key[-1], "d": key[3] if len(key) > 4 else 0}[key[0]]
        made = self.coming.pop(key, None)
        if made is not None:
            for one, (when, _) in zip(made, self.widths(self.last(slot))):
                if when is None:
                    one.wait_recv()
                else:
                    pl.when(when)(one.wait_recv)

    def spread(self, j, zr):
        links = self.links
        if zr == 0:
            for at, when, wait in self.own:
                if at == j:
                    wait() if when is None else pl.when(when)(wait)
        else:
            self.arrive("z", j, zr)
        last = self.last(0)
        for dx in range(1, links.nx):
            self.pass_on(
                ("x", j, zr, dx),
                j,
                lambda width: self.spot(j, zr, 0, 0, width),
                lambda width: self.spot(j, zr, 0, dx, width),
                self.x_sem,
                (j, zr, dx - 1),
                links.far(dx=dx),
                last,
            )
        for dy in range(1, links.ny):
            self.pass_on(
                ("y", j, zr, dy),
                j,
                lambda width: self.spot(j, zr, 0, 0, width),
                lambda width: self.spot(j, zr, 0, 0, width),
                self.y_sem,
                (j, zr, dy - 1),
                links.far(dy=dy),
                last,
            )

    def relay(self, j, zr):
        links = self.links
        over_y = (j + zr) % 2 == 0
        for dx in range(1, links.nx):
            if over_y:
                self.arrive("x", j, zr, dx)
            for dy in range(1, links.ny):
                if not over_y:
                    self.arrive("y", j, zr, dy)
                slot, shift = (dx, 0) if over_y else (0, dy)
                self.pass_on(
                    ("d", j, zr, dx, dy),
                    j,
                    lambda width: self.spot(j, zr, shift, slot, width),
                    lambda width: self.spot(j, zr, shift, dx, width),
                    self.d_sem,
                    (j, zr, dx - 1, dy - 1),
                    links.far(dy=dy) if over_y else links.far(dx=dx),
                    self.last(slot),
                )

    def need(self, j, zr):
        for key in [key for key in self.coming if key[1:3] == (j, zr)]:
            self.arrive(*key)


def layer_kernel(
    n,
    nt,
    nz,
    u,
    added,
    lines,
    entry,
    read,
    residual,
    weight,
    mix_gain,
    pre_gain,
    post_gain,
    gate_weight,
    up_weight,
    down_weight,
    out,
    mag,
    dr,
    di,
    ends,
    send,
    recv,
    start,
    active,
    part,
    pair_land,
    half,
    half_land,
    staged,
    held,
    rows_all,
    hidden,
    other,
    other_land,
    sums,
    sums_send,
    sums_land,
    send_sem,
    recv_sem,
    local_sem,
    z_sem,
    x_sem,
    y_sem,
    d_sem,
    pair_sem,
    half_sem,
    row_sem,
    row_pair_sem,
    other_sem,
    sums_sem,
):
    me = lax.axis_index("sp")
    links = Links(n, nt, nz)
    nx, nc, ny = links.nx, links.nc, links.ny
    rows, flat = dr.shape
    own = rows // nt
    steps = rows // CHUNKS
    states, width = flat // added.shape[1], entry.shape[1]
    pack = LANES // width
    packs, wide = added.shape[1] // pack, pack * states
    block = min(BLOCK, flat)

    barrier = pltpu.get_barrier_semaphore()
    for d in range(1, n):
        pl.semaphore_signal(
            barrier, inc=1, device_id={"sp": lax.rem(me + d, n)}, device_id_type=MESH
        )
    place = lax.axis_index("tp")
    for d in range(1, nt):
        pl.semaphore_signal(
            barrier, inc=1, device_id={"tp": lax.rem(place + d, nt)}, device_id_type=MESH
        )
    weights = Weights(
        links, (gate_weight, up_weight, down_weight), staged, held, local_sem, z_sem, x_sem, y_sem, d_sem
    )
    weights.begin()
    pl.semaphore_wait(barrier, n - 1 + nt - 1)
    near, far = range(1, min(2, nz)), range(2, nz)

    def each(step, j, reach):
        for zr in reach:
            step(j, zr)

    each(weights.along_z, 0, near)
    weights.spread(0, 0)
    weights.clear()

    down = lax.broadcasted_iota(jnp.int32, (rows, rows), 0)
    over = lax.broadcasted_iota(jnp.int32, (rows, rows), 1)
    mixing = one_hot(over == lax.rem(down, CHUNKS) * steps + lax.div(down, CHUNKS))
    order = one_hot(over == lax.rem(down, steps) * CHUNKS + lax.div(down, steps))
    mixed_u = dot32(mixing, u[...]).astype(jnp.bfloat16)
    groups = added.shape[1]
    repeat = one_hot(
        lax.div(lax.broadcasted_iota(jnp.int32, (groups, flat), 1), states)
        == lax.broadcasted_iota(jnp.int32, (groups, flat), 0)
    )
    rest = jnp.exp(added[...])
    total = None
    for _ in range(3):
        term = rest.astype(jnp.bfloat16)
        rest = rest - term.astype(jnp.float32)
        term = dot32(dot32(mixing, term).astype(jnp.bfloat16), repeat)
        total = term if total is None else total + term
    mag[...] = total
    same = lax.div(
        lax.broadcasted_iota(jnp.int32, (LANES, wide), 0), width
    ) == lax.div(lax.broadcasted_iota(jnp.int32, (LANES, wide), 1), states)

    def blocks(rows_of_channels):
        return jnp.where(same, jnp.concatenate([rows_of_channels] * pack, axis=0), 0.0)

    cr, ci = lines.at[0:1], lines.at[1:2]
    for p in range(packs):
        at = pl.ds(p * wide, wide)
        piece = mixed_u[:, p * LANES : (p + 1) * LANES]
        ratio = times(lines[2:3, at], lines[3:4, at], entry[0, :, at], entry[1, :, at])
        for bar, dst in zip(ratio, (dr, di)):
            high, low = split(blocks(bar))
            dst[:, at] = dot32(piece, high) + dot32(piece, low)

    for b in range(0, flat, block):
        at = pl.ds(b, block)
        kr = jnp.broadcast_to(cr[0:1, at], (CHUNKS, block))
        ki = jnp.broadcast_to(ci[0:1, at], (CHUNKS, block))

        def first(j, held_values):
            pr, pi, sr, si = held_values
            row = pl.ds(pl.multiple_of(j * CHUNKS, CHUNKS), CHUNKS)
            m = mag[row, at]
            ar, ai = m * kr, m * ki
            pr, pi = times(ar, ai, pr, pi)
            sr, si = times(ar, ai, sr, si)
            return pr, pi, sr + dr[row, at], si + di[row, at]

        zero = jnp.zeros((CHUNKS, block), jnp.float32)
        values = lax.fori_loop(0, steps, first, (zero + 1.0, zero, zero, zero), unroll=2)
        for k in range(4):
            ends[k, :, at] = values[k]

    pr, pi, sr, si = (ends[k, 0:1, :] for k in range(4))
    for c in range(1, CHUNKS):
        ar, ai, br, bi = (ends[k, c : c + 1, :] for k in range(4))
        pr, pi = times(ar, ai, pr, pi)
        sr, si = times(ar, ai, sr, si)
        sr, si = sr + br, si + bi
    for k, item in enumerate((pr, pi, sr, si)):
        send[k : k + 1, :] = item[:, : flat // 2]
        send[4 + k : 5 + k, :] = item[:, flat // 2 :]

    copies = []
    for d in range(1, n):
        copy = pltpu.make_async_remote_copy(
            src_ref=send,
            dst_ref=recv.at[me],
            send_sem=send_sem.at[d - 1],
            recv_sem=recv_sem.at[d - 1],
            device_id={"sp": lax.rem(me + d, n)},
            device_id_type=MESH,
        )
        pl.when(me + d < n)(copy.start)
        copies.append(copy)

    for d, copy in enumerate(copies, 1):
        pl.when(me >= d)(copy.wait_recv)
    weights.spread(1, 0)
    weights.spread(2, 0)
    weights.relay(0, 0)

    sr = jnp.zeros((1, flat), jnp.float32)
    si = sr
    for k in range(n - 1):
        ar, ai, br, bi = (
            jnp.concatenate([recv[k, q : q + 1, :], recv[k, 4 + q : 5 + q, :]], axis=1)
            for q in range(4)
        )
        nr, ni = times(ar, ai, sr, si)
        sr = jnp.where(k < me, nr + br, sr)
        si = jnp.where(k < me, ni + bi, si)
    for c in range(CHUNKS):
        start[0, c : c + 1, :] = sr
        start[1, c : c + 1, :] = si
        ar, ai, br, bi = (ends[k, c : c + 1, :] for k in range(4))
        sr, si = times(ar, ai, sr, si)
        sr, si = sr + br, si + bi

    for b in range(0, flat, block):
        at = pl.ds(b, block)
        kr = jnp.broadcast_to(cr[0:1, at], (CHUNKS, block))
        ki = jnp.broadcast_to(ci[0:1, at], (CHUNKS, block))

        def second(j, held_values):
            row = pl.ds(pl.multiple_of(j * CHUNKS, CHUNKS), CHUNKS)
            m = mag[row, at]
            sr, si = times(m * kr, m * ki, *held_values)
            sr, si = sr + dr[row, at], si + di[row, at]
            dr[row, at] = sr
            di[row, at] = si
            return sr, si

        lax.fori_loop(0, steps, second, (start[0, :, at], start[1, :, at]), unroll=2)

    for p in range(packs):
        total = None
        at = pl.ds(p * wide, wide)
        for state, part_read in ((dr, read[0, :, at]), (di, -read[1, :, at])):
            high, low = split(state[:, at])
            top, rest = split(blocks(part_read))
            term = across(high, top) + across(high, rest) + across(low, top)
            total = term if total is None else total + term
        active[:, p * LANES : (p + 1) * LANES] = jax.nn.gelu(total).astype(jnp.bfloat16)

    active[...] = dot32(order, active[...]).astype(jnp.bfloat16)
    columns = weight.shape[1]
    for b in range(0, columns, BLOCK):
        at = pl.ds(b, BLOCK)
        part[:, at] = dot32(active[...], weight[:, at]).astype(jnp.bfloat16)

    each(weights.along_z, 0, far)
    each(weights.along_z, 1, near)

    def rows_of(x, c):
        return span(x * nc + c, own)

    pairs = []
    for dc in range(1, nc):
        for x in range(nx):
            pairs.append(
                links.copy(
                    part.at[rows_of(x, lax.rem(links.c + dc, nc))],
                    pair_land.at[dc - 1, x],
                    pair_sem,
                    (dc - 1, x),
                    links.far(dc=dc),
                )
            )
    for made in pairs:
        made.wait_recv()

    def chip_sum(x):
        value = part[rows_of(x, links.c), :].astype(jnp.float32)
        for dc in range(1, nc):
            value = value + pair_land[dc - 1, x].astype(jnp.float32)
        return value

    halves = []
    for dx in range(1, nx):
        half[dx - 1] = chip_sum(lax.rem(links.x + dx, nx)).astype(jnp.bfloat16)
        halves.append(
            links.copy(half.at[dx - 1], half_land.at[dx - 1], half_sem, (dx - 1,), links.far(dx=dx))
        )
    each(weights.spread, 0, near)
    weights.relay(1, 0)
    weights.relay(2, 0)
    mixed = chip_sum(links.x)
    for dx, made in enumerate(halves):
        made.wait_recv()
        mixed = mixed + half_land[dx].astype(jnp.float32)
    middle = (residual[...].astype(jnp.float32) + rms_scale(mixed, mix_gain[...])).astype(
        jnp.bfloat16
    )
    line = nz * own
    bits = [1 << k for k in range(nz.bit_length() - 1)]
    rows_all[:own] = rms_scale(middle.astype(jnp.float32), pre_gain[...]).astype(jnp.bfloat16)
    along = {}
    to_pair = []

    def row_block(zr, dc=0):
        return pl.ds(dc * line + mirror(zr, nz) * own, own)

    def hand_on(zr):
        if zr:
            along[zr].wait_recv()
        for bit in reversed(bits):
            if zr == 0 or bit < (zr & -zr):
                along[zr ^ bit] = links.copy(
                    rows_all.at[row_block(zr)],
                    rows_all.at[row_block(zr ^ bit)],
                    row_sem,
                    ((zr ^ bit) - 1,),
                    links.far(dz=bit),
                )
        for dc in range(1, nc):
            to_pair.append(
                links.copy(
                    rows_all.at[row_block(zr)],
                    rows_all.at[row_block(zr, dc)],
                    row_pair_sem,
                    (zr, dc - 1),
                    links.far(dc=dc),
                )
            )

    hand_on(0)
    each(weights.spread, 0, far)
    each(weights.relay, 0, near)
    meanwhile = [
        [
            (weights.along_z, 1, far),
            (weights.relay, 0, far),
            (weights.spread, 1, near),
            (weights.relay, 1, near),
        ],
        [],
        [(weights.along_z, 2, range(1, nz))],
    ]
    for zr in sorted(range(1, nz), key=lambda zr: -(zr & -zr)):
        hand_on(zr)
        for item in meanwhile.pop(0) if meanwhile else ():
            each(*item)
    for items in meanwhile:
        for item in items:
            each(*item)
    each(weights.spread, 1, far)
    each(weights.relay, 1, far)
    each(weights.spread, 2, near)
    each(weights.relay, 2, near)
    for made in to_pair:
        made.wait_recv()
    for j in range(2):
        for zr in range(nz):
            weights.need(j, zr)

    valid = []
    for slot in range(nx):
        at = lax.broadcasted_iota(jnp.int32, (1, weights.wide), 1)
        limit = jnp.where(weights.last(slot), weights.thin, weights.wide)
        valid.append(jnp.where(at < limit, 1.0, 0.0))
    valid = jnp.concatenate(valid, axis=1)

    def mix(b, carry):
        at = span(b, line)
        gate = dot32(rows_all[at, :], held[0])
        up = dot32(rows_all[at, :], held[1])
        hidden[at, :] = jnp.where(valid > 0.0, jax.nn.silu(gate) * up, 0.0).astype(jnp.bfloat16)
        return carry

    lax.fori_loop(0, nc, mix, 0)
    each(weights.spread, 2, far)

    slab = ny * weights.depth
    others = {}
    parts = {}

    def place_of(q):
        return span(flip(links.z, q), slab)

    def project(q):
        weights.need(2, q)
        at = place_of(q)
        value = across(hidden[...], held[2, at, :])
        sums[:, at] = value[:line]
        for dc in range(1, nc):
            other[dc - 1, :, at] = value[dc * line : (dc + 1) * line].astype(jnp.bfloat16)
            others[q, dc] = links.copy(
                other.at[dc - 1, :, at],
                other_land.at[dc - 1, :, at],
                other_sem,
                (q, dc - 1),
                links.far(dc=nc - dc),
            )

    def give(q, level, value):
        if level == len(bits):
            sums[:own, place_of(q)] = value
            return
        at = place_of(q)
        count = value.shape[0] // 2
        half_rows = pl.ds(count, count)
        sums[:count, at] = value[:count]
        sums_send[half_rows, at] = value[count:].astype(jnp.bfloat16)
        parts[q ^ bits[level], level] = links.copy(
            sums_send.at[half_rows, at],
            sums_land.at[half_rows, at],
            sums_sem,
            (q ^ bits[level], level),
            links.far(dz=bits[level]),
        )

    def take(q, level):
        at = place_of(q)
        count = line >> (level + 1)
        parts[q, level].wait_recv()
        land = sums_land[pl.ds(count, count), at].astype(jnp.float32)
        give(q, level + 1, sums[:count, at] + land)

    def settle(q):
        at = place_of(q)
        value = sums[:, at]
        for dc in range(1, nc):
            others[q, dc].wait_recv()
            value = value + other_land[dc - 1, :, at].astype(jnp.float32)
        give(q, 0, value)

    ready = min(2, nz)
    for q in range(ready):
        project(q)
    for q in range(ready):
        settle(q)
    each(weights.relay, 2, far)
    if bits:
        for q in range(ready):
            take(q, 0)
    for q in range(ready, nz):
        project(q)
    for q in range(ready, nz):
        settle(q)
    for q in range(ready, nz):
        take(q, 0)
    for level in range(1, len(bits)):
        for q in range(nz):
            take(q, level)
    total = sums[:own, :]
    out[...] = (middle.astype(jnp.float32) + 0.5 * rms_scale(total, post_gain[...])).astype(
        jnp.bfloat16
    )
    for wait in links.sent:
        wait()
    for d, copy in enumerate(copies, 1):
        pl.when(me + d < n)(copy.wait_send)


def shards(
    n,
    nt,
    residual,
    inputs,
    pole_real,
    pole_imaginary,
    step_log,
    input_real,
    entry_map_quadrature,
    output_real,
    output_imaginary,
    added_log_decay,
    out_weight,
    mix_gain,
    gate_weight,
    up_weight,
    down_weight,
    pre_gain,
    post_gain,
):
    rows, channels = inputs.shape
    columns = out_weight.shape[1]
    groups, states = pole_real.shape
    width = input_real.shape[2]
    flat = groups * states
    step_size = jnp.exp(step_log)[:, None]
    log_size = pole_real * step_size
    angle = pole_imaginary * step_size
    cosine = jnp.cos(angle)
    sine = jnp.sin(angle)
    magnitude = jnp.exp(log_size)
    lift_real = jnp.expm1(log_size) * cosine - 2.0 * jnp.sin(0.5 * angle) ** 2
    lift_imaginary = magnitude * sine
    denominator = pole_real * pole_real + pole_imaginary * pole_imaginary
    ratio_real = (lift_real * pole_real + lift_imaginary * pole_imaginary) / denominator
    ratio_imaginary = (lift_imaginary * pole_real - lift_real * pole_imaginary) / denominator
    lines = jnp.stack(
        (magnitude * cosine, magnitude * sine, ratio_real, ratio_imaginary)
    ).reshape(4, flat)
    entry = jnp.stack((input_real, entry_map_quadrature)).transpose(0, 3, 1, 2)
    read = jnp.stack((output_real, output_imaginary)).transpose(0, 2, 1, 3)
    vmem = pl.BlockSpec(memory_space=pltpu.VMEM)
    nz = math.gcd(n, nt)
    nz = nz & -nz
    ny, nx = n // nz, nt // CORES
    own = rows // nt
    line = nz * own
    depth, units = gate_weight.shape
    piece = -(-units // (LANES * nz)) * LANES
    bf, f32 = jnp.bfloat16, jnp.float32
    return pl.pallas_call(
        functools.partial(layer_kernel, n, nt, nz),
        out_shape=jax.ShapeDtypeStruct((own, columns), bf),
        in_specs=[vmem] * 10 + [pl.BlockSpec(memory_space=pl.ANY)] * 3,
        out_specs=vmem,
        scratch_shapes=[
            pltpu.VMEM((rows, flat), f32),
            pltpu.VMEM((rows, flat), f32),
            pltpu.VMEM((rows, flat), f32),
            pltpu.VMEM((4, CHUNKS, flat), f32),
            pltpu.VMEM((8, flat // 2), f32),
            pltpu.VMEM((n, 8, flat // 2), f32),
            pltpu.VMEM((2, CHUNKS, flat), f32),
            pltpu.VMEM((rows, channels), bf),
            pltpu.VMEM((rows, columns), bf),
            pltpu.VMEM((CORES - 1, nx, own, columns), bf),
            pltpu.VMEM((nx - 1, own, columns), bf),
            pltpu.VMEM((nx - 1, own, columns), bf),
            pltpu.VMEM((3, depth, units), bf),
            pltpu.VMEM((3, n * depth, nx * piece), bf),
            pltpu.VMEM((CORES * line, columns), bf),
            pltpu.VMEM((CORES * line, nx * piece), bf),
            pltpu.VMEM((CORES - 1, line, columns), bf),
            pltpu.VMEM((CORES - 1, line, columns), bf),
            pltpu.VMEM((line, columns), f32),
            pltpu.VMEM((line, columns), bf),
            pltpu.VMEM((line, columns), bf),
            pltpu.SemaphoreType.DMA((n - 1,)),
            pltpu.SemaphoreType.DMA((n - 1,)),
            pltpu.SemaphoreType.DMA((2, 3)),
            pltpu.SemaphoreType.DMA((2, 3, nz - 1)),
            pltpu.SemaphoreType.DMA((2, 3, nz, nx - 1)),
            pltpu.SemaphoreType.DMA((2, 3, nz, ny - 1)),
            pltpu.SemaphoreType.DMA((2, 3, nz, nx - 1, ny - 1)),
            pltpu.SemaphoreType.DMA((2, CORES - 1, nx)),
            pltpu.SemaphoreType.DMA((2, nx - 1)),
            pltpu.SemaphoreType.DMA((2, nz - 1)),
            pltpu.SemaphoreType.DMA((2, nz, CORES - 1)),
            pltpu.SemaphoreType.DMA((2, nz, CORES - 1)),
            pltpu.SemaphoreType.DMA((2, nz, nz.bit_length())),
        ],
        compiler_params=pltpu.CompilerParams(
            collective_id=0, has_side_effects=True, vmem_limit_bytes=60 * 1024 * 1024
        ),
    )(
        inputs,
        added_log_decay,
        lines,
        entry.reshape(2, width, flat),
        read.reshape(2, width, flat),
        residual,
        out_weight,
        mix_gain.reshape(1, columns),
        pre_gain.reshape(1, columns),
        post_gain.reshape(1, columns),
        gate_weight,
        up_weight,
        down_weight,
    )


def solution(mesh):
    return jax.shard_map(
        functools.partial(shards, mesh.shape["sp"], mesh.shape["tp"]),
        mesh=mesh,
        in_specs=(
            P(("sp", "tp"), None),
            P("sp", "tp"),
            P("tp", None),
            P("tp", None),
            P("tp"),
            P("tp", None, None),
            P("tp", None, None),
            P("tp", None, None),
            P("tp", None, None),
            P("sp", "tp"),
            P("tp", None),
            P(),
            P("sp", "tp"),
            P("sp", "tp"),
            P("sp", "tp"),
            P(),
            P(),
        ),
        out_specs=P(("sp", "tp"), None),
        check_vma=False,
    )
```

```python
import functools
import math

import jax
import jax.numpy as jnp
from jax import lax
from jax.experimental import pallas as pl
from jax.experimental.pallas import tpu as pltpu
from jax.sharding import PartitionSpec as P

EPSILON = 1e-06
CHUNKS = 8
LANES = 128
BLOCK = 512
CORES = 2
MESH = pl.DeviceIdType.MESH


def rms_scale(values, gain):
    return values * lax.rsqrt(jnp.mean(values * values, axis=-1, keepdims=True) + EPSILON) * gain


def split(values):
    high = values.astype(jnp.bfloat16)
    return high, (values - high.astype(jnp.float32)).astype(jnp.bfloat16)


def dot32(a, b):
    return jnp.dot(a, b, preferred_element_type=jnp.float32)


def times(ar, ai, br, bi):
    return ar * br - ai * bi, ar * bi + ai * br


def flip(index, mask):
    out, bit = index, 1
    while bit <= mask:
        if mask & bit:
            out = out + bit - 2 * bit * lax.rem(lax.div(index, bit), 2)
        bit *= 2
    return out


def mirror(place, size):
    out = 0
    while size > 1:
        out, place, size = 2 * out + place % 2, place // 2, size // 2
    return out


def across(a, b):
    return lax.dot_general(
        a, b, (((1,), (1,)), ((), ())), preferred_element_type=jnp.float32
    )


def one_hot(where):
    return jnp.where(where, 1.0, 0.0).astype(jnp.bfloat16)


class Links:
    def __init__(self, n, nt, nz):
        self.nz, self.ny, self.nx, self.nc = nz, n // nz, nt // CORES, CORES
        sp, tp = lax.axis_index("sp"), lax.axis_index("tp")
        self.z, self.y = lax.div(sp, self.ny), lax.rem(sp, self.ny)
        self.x, self.c = lax.div(tp, self.nc), lax.rem(tp, self.nc)
        self.sent = []

    def far(self, dz=0, dy=0, dx=0, dc=0):
        return {
            "sp": flip(self.z, dz) * self.ny + lax.rem(self.y + dy, self.ny),
            "tp": lax.rem(self.x + dx, self.nx) * self.nc + lax.rem(self.c + dc, self.nc),
        }

    def copy(self, src, dst, sems, index, device, when=None):
        made = pltpu.make_async_remote_copy(
            src_ref=src,
            dst_ref=dst,
            send_sem=sems.at[(0,) + index],
            recv_sem=sems.at[(1,) + index],
            device_id=device,
            device_id_type=MESH,
        )
        if when is None:
            made.start()
            self.sent.append(made.wait_send)
        else:
            pl.when(when)(made.start)
            self.sent.append(lambda: pl.when(when)(made.wait_send))
        return made


def span(index, size):
    return pl.ds(pl.multiple_of(index * size, size), size)


class Weights:
    def __init__(self, links, sources, staged, held, local, z_sem, x_sem, y_sem, d_sem):
        self.links, self.sources, self.staged, self.held = links, sources, staged, held
        self.local, self.z_sem, self.x_sem, self.y_sem, self.d_sem = (
            local,
            z_sem,
            x_sem,
            y_sem,
            d_sem,
        )
        self.depth, self.units = sources[0].shape
        self.wide = held.shape[2] // links.nx
        self.thin = self.units - (links.nz - 1) * self.wide
        self.coming = {}

    def piece(self, z, x):
        links = self.links
        nt = links.nx * links.nc
        tp = x * links.nc + links.c
        return lax.rem(z + links.nz * nt - tp - 1, links.nz)

    def last(self, slot):
        links = self.links
        return self.piece(links.z, lax.rem(links.x - slot + links.nx, links.nx)) == links.nz - 1

    def widths(self, last):
        if self.thin == self.wide:
            return ((None, self.wide),)
        return ((jnp.logical_not(last), self.wide), (last, self.thin))

    def spot(self, j, zr, dy, slot, width):
        links = self.links
        origin = flip(links.z, zr) * links.ny + lax.rem(links.y - dy + links.ny, links.ny)
        return self.held.at[j, span(origin, self.depth), pl.ds(slot * self.wide, width)]

    def cut(self, source, which, width):
        first = jnp.minimum(which * self.wide, self.units - width)
        return source.at[:, pl.ds(pl.multiple_of(first, LANES), width)]

    def begin(self):
        links = self.links
        which = self.piece(links.z, links.x)
        self.own = []
        self.whole = [
            pltpu.make_async_copy(source, self.staged.at[j], self.local.at[1, j])
            for j, source in enumerate(self.sources)
        ]
        for j in range(len(self.sources)):
            self.whole[j].start()
            for when, width in self.widths(which == links.nz - 1):
                own = pltpu.make_async_copy(
                    self.cut(self.sources[j], which, width),
                    self.spot(j, 0, 0, 0, width),
                    self.local.at[0, j],
                )
                if when is None:
                    own.start()
                else:
                    pl.when(when)(own.start)
                self.own.append((j, when, own.wait))

    def clear(self):
        if self.thin < self.wide:
            for slot in range(self.links.nx):

                @pl.when(self.last(slot))
                def _():
                    at = pl.ds(slot * self.wide + self.thin, self.wide - self.thin)
                    self.held[2, :, at] = jnp.zeros(
                        (self.held.shape[1], self.wide - self.thin), self.held.dtype
                    )

    def pass_on(self, key, j, source, target, sems, index, device, last):
        for when, width in self.widths(last):
            made = self.links.copy(source(width), target(width), sems, index, device, when)
            self.coming.setdefault(key, []).append(made)

    def along_z(self, j, zr):
        links = self.links
        which = self.piece(flip(links.z, zr), links.x)
        if zr == 1:
            self.whole[j].wait()
        self.pass_on(
            ("z", j, zr),
            j,
            lambda width: self.cut(self.staged.at[j], which, width),
            lambda width: self.spot(j, 0, 0, 0, width),
            self.z_sem,
            (j, zr - 1),
            links.far(dz=zr),
            which == links.nz - 1,
        )

    def arrive(self, *key):
        slot = {"z": 0, "y": 0, "x": key[-1], "d": key[3] if len(key) > 4 else 0}[key[0]]
        made = self.coming.pop(key, None)
        if made is not None:
            for one, (when, _) in zip(made, self.widths(self.last(slot))):
                if when is None:
                    one.wait_recv()
                else:
                    pl.when(when)(one.wait_recv)

    def spread(self, j, zr):
        links = self.links
        if zr == 0:
            for at, when, wait in self.own:
                if at == j:
                    wait() if when is None else pl.when(when)(wait)
        else:
            self.arrive("z", j, zr)
        last = self.last(0)
        for dx in range(1, links.nx):
            self.pass_on(
                ("x", j, zr, dx),
                j,
                lambda width: self.spot(j, zr, 0, 0, width),
                lambda width: self.spot(j, zr, 0, dx, width),
                self.x_sem,
                (j, zr, dx - 1),
                links.far(dx=dx),
                last,
            )
        for dy in range(1, links.ny):
            self.pass_on(
                ("y", j, zr, dy),
                j,
                lambda width: self.spot(j, zr, 0, 0, width),
                lambda width: self.spot(j, zr, 0, 0, width),
                self.y_sem,
                (j, zr, dy - 1),
                links.far(dy=dy),
                last,
            )

    def relay(self, j, zr):
        links = self.links
        over_y = (j + zr) % 2 == 0
        for dx in range(1, links.nx):
            if over_y:
                self.arrive("x", j, zr, dx)
            for dy in range(1, links.ny):
                if not over_y:
                    self.arrive("y", j, zr, dy)
                slot, shift = (dx, 0) if over_y else (0, dy)
                self.pass_on(
                    ("d", j, zr, dx, dy),
                    j,
                    lambda width: self.spot(j, zr, shift, slot, width),
                    lambda width: self.spot(j, zr, shift, dx, width),
                    self.d_sem,
                    (j, zr, dx - 1, dy - 1),
                    links.far(dy=dy) if over_y else links.far(dx=dx),
                    self.last(slot),
                )

    def need(self, j, zr):
        for key in [key for key in self.coming if key[1:3] == (j, zr)]:
            self.arrive(*key)


def layer_kernel(
    n,
    nt,
    nz,
    u,
    added,
    lines,
    entry,
    read,
    residual,
    weight,
    mix_gain,
    pre_gain,
    post_gain,
    gate_weight,
    up_weight,
    down_weight,
    out,
    mag,
    dr,
    di,
    ends,
    send,
    recv,
    start,
    active,
    part,
    pair_land,
    half,
    half_land,
    staged,
    held,
    rows_all,
    hidden,
    other,
    other_land,
    sums,
    sums_send,
    sums_land,
    send_sem,
    recv_sem,
    local_sem,
    z_sem,
    x_sem,
    y_sem,
    d_sem,
    pair_sem,
    half_sem,
    row_sem,
    row_pair_sem,
    other_sem,
    sums_sem,
):
    me = lax.axis_index("sp")
    links = Links(n, nt, nz)
    nx, nc, ny = links.nx, links.nc, links.ny
    rows, flat = dr.shape
    own = rows // nt
    steps = rows // CHUNKS
    states, width = flat // added.shape[1], entry.shape[1]
    pack = LANES // width
    packs, wide = added.shape[1] // pack, pack * states
    block = min(BLOCK, flat)

    barrier = pltpu.get_barrier_semaphore()
    for d in range(1, n):
        pl.semaphore_signal(
            barrier, inc=1, device_id={"sp": lax.rem(me + d, n)}, device_id_type=MESH
        )
    place = lax.axis_index("tp")
    for d in range(1, nt):
        pl.semaphore_signal(
            barrier, inc=1, device_id={"tp": lax.rem(place + d, nt)}, device_id_type=MESH
        )
    weights = Weights(
        links, (gate_weight, up_weight, down_weight), staged, held, local_sem, z_sem, x_sem, y_sem, d_sem
    )
    weights.begin()
    pl.semaphore_wait(barrier, n - 1 + nt - 1)
    near, far = range(1, min(2, nz)), range(2, nz)

    def each(step, j, reach):
        for zr in reach:
            step(j, zr)

    each(weights.along_z, 0, near)
    weights.spread(0, 0)
    weights.clear()

    down = lax.broadcasted_iota(jnp.int32, (rows, rows), 0)
    over = lax.broadcasted_iota(jnp.int32, (rows, rows), 1)
    mixing = one_hot(over == lax.rem(down, CHUNKS) * steps + lax.div(down, CHUNKS))
    order = one_hot(over == lax.rem(down, steps) * CHUNKS + lax.div(down, steps))
    mixed_u = dot32(mixing, u[...]).astype(jnp.bfloat16)
    groups = added.shape[1]
    repeat = one_hot(
        lax.div(lax.broadcasted_iota(jnp.int32, (groups, flat), 1), states)
        == lax.broadcasted_iota(jnp.int32, (groups, flat), 0)
    )
    rest = jnp.exp(added[...])
    total = None
    for _ in range(3):
        term = rest.astype(jnp.bfloat16)
        rest = rest - term.astype(jnp.float32)
        term = dot32(dot32(mixing, term).astype(jnp.bfloat16), repeat)
        total = term if total is None else total + term
    mag[...] = total
    same = lax.div(
        lax.broadcasted_iota(jnp.int32, (LANES, wide), 0), width
    ) == lax.div(lax.broadcasted_iota(jnp.int32, (LANES, wide), 1), states)

    def blocks(rows_of_channels):
        return jnp.where(same, jnp.concatenate([rows_of_channels] * pack, axis=0), 0.0)

    cr, ci = lines.at[0:1], lines.at[1:2]
    for p in range(packs):
        at = pl.ds(p * wide, wide)
        piece = mixed_u[:, p * LANES : (p + 1) * LANES]
        ratio = times(lines[2:3, at], lines[3:4, at], entry[0, :, at], entry[1, :, at])
        for bar, dst in zip(ratio, (dr, di)):
            high, low = split(blocks(bar))
            dst[:, at] = dot32(piece, high) + dot32(piece, low)

    for b in range(0, flat, block):
        at = pl.ds(b, block)
        kr = jnp.broadcast_to(cr[0:1, at], (CHUNKS, block))
        ki = jnp.broadcast_to(ci[0:1, at], (CHUNKS, block))

        def first(j, held_values):
            pr, pi, sr, si = held_values
            row = pl.ds(pl.multiple_of(j * CHUNKS, CHUNKS), CHUNKS)
            m = mag[row, at]
            ar, ai = m * kr, m * ki
            pr, pi = times(ar, ai, pr, pi)
            sr, si = times(ar, ai, sr, si)
            return pr, pi, sr + dr[row, at], si + di[row, at]

        zero = jnp.zeros((CHUNKS, block), jnp.float32)
        values = lax.fori_loop(0, steps, first, (zero + 1.0, zero, zero, zero), unroll=2)
        for k in range(4):
            ends[k, :, at] = values[k]

    pr, pi, sr, si = (ends[k, 0:1, :] for k in range(4))
    for c in range(1, CHUNKS):
        ar, ai, br, bi = (ends[k, c : c + 1, :] for k in range(4))
        pr, pi = times(ar, ai, pr, pi)
        sr, si = times(ar, ai, sr, si)
        sr, si = sr + br, si + bi
    for k, item in enumerate((pr, pi, sr, si)):
        send[k : k + 1, :] = item[:, : flat // 2]
        send[4 + k : 5 + k, :] = item[:, flat // 2 :]

    copies = []
    for d in range(1, n):
        copy = pltpu.make_async_remote_copy(
            src_ref=send,
            dst_ref=recv.at[me],
            send_sem=send_sem.at[d - 1],
            recv_sem=recv_sem.at[d - 1],
            device_id={"sp": lax.rem(me + d, n)},
            device_id_type=MESH,
        )
        pl.when(me + d < n)(copy.start)
        copies.append(copy)

    for d, copy in enumerate(copies, 1):
        pl.when(me >= d)(copy.wait_recv)
    weights.spread(1, 0)
    weights.spread(2, 0)
    weights.relay(0, 0)

    sr = jnp.zeros((1, flat), jnp.float32)
    si = sr
    for k in range(n - 1):
        ar, ai, br, bi = (
            jnp.concatenate([recv[k, q : q + 1, :], recv[k, 4 + q : 5 + q, :]], axis=1)
            for q in range(4)
        )
        nr, ni = times(ar, ai, sr, si)
        sr = jnp.where(k < me, nr + br, sr)
        si = jnp.where(k < me, ni + bi, si)
    for c in range(CHUNKS):
        start[0, c : c + 1, :] = sr
        start[1, c : c + 1, :] = si
        ar, ai, br, bi = (ends[k, c : c + 1, :] for k in range(4))
        sr, si = times(ar, ai, sr, si)
        sr, si = sr + br, si + bi

    for b in range(0, flat, block):
        at = pl.ds(b, block)
        kr = jnp.broadcast_to(cr[0:1, at], (CHUNKS, block))
        ki = jnp.broadcast_to(ci[0:1, at], (CHUNKS, block))

        def second(j, held_values):
            row = pl.ds(pl.multiple_of(j * CHUNKS, CHUNKS), CHUNKS)
            m = mag[row, at]
            sr, si = times(m * kr, m * ki, *held_values)
            sr, si = sr + dr[row, at], si + di[row, at]
            dr[row, at] = sr
            di[row, at] = si
            return sr, si

        lax.fori_loop(0, steps, second, (start[0, :, at], start[1, :, at]), unroll=2)

    for p in range(packs):
        total = None
        at = pl.ds(p * wide, wide)
        for state, part_read in ((dr, read[0, :, at]), (di, -read[1, :, at])):
            high, low = split(state[:, at])
            top, rest = split(blocks(part_read))
            term = across(high, top) + across(high, rest) + across(low, top)
            total = term if total is None else total + term
        active[:, p * LANES : (p + 1) * LANES] = jax.nn.gelu(total).astype(jnp.bfloat16)

    active[...] = dot32(order, active[...]).astype(jnp.bfloat16)
    columns = weight.shape[1]
    for b in range(0, columns, BLOCK):
        at = pl.ds(b, BLOCK)
        part[:, at] = dot32(active[...], weight[:, at]).astype(jnp.bfloat16)

    each(weights.along_z, 0, far)
    each(weights.along_z, 1, near)
    each(weights.along_z, 2, near)

    def rows_of(x, c):
        return span(x * nc + c, own)

    pairs = []
    for dc in range(1, nc):
        for x in range(nx):
            pairs.append(
                links.copy(
                    part.at[rows_of(x, lax.rem(links.c + dc, nc))],
                    pair_land.at[dc - 1, x],
                    pair_sem,
                    (dc - 1, x),
                    links.far(dc=dc),
                )
            )
    for made in pairs:
        made.wait_recv()

    def chip_sum(x):
        value = part[rows_of(x, links.c), :].astype(jnp.float32)
        for dc in range(1, nc):
            value = value + pair_land[dc - 1, x].astype(jnp.float32)
        return value

    halves = []
    for dx in range(1, nx):
        half[dx - 1] = chip_sum(lax.rem(links.x + dx, nx)).astype(jnp.bfloat16)
        halves.append(
            links.copy(half.at[dx - 1], half_land.at[dx - 1], half_sem, (dx - 1,), links.far(dx=dx))
        )
    each(weights.spread, 0, near)
    weights.relay(1, 0)
    weights.relay(2, 0)
    mixed = chip_sum(links.x)
    for dx, made in enumerate(halves):
        made.wait_recv()
        mixed = mixed + half_land[dx].astype(jnp.float32)
    middle = (residual[...].astype(jnp.float32) + rms_scale(mixed, mix_gain[...])).astype(
        jnp.bfloat16
    )
    line = nz * own
    bits = [1 << k for k in range(nz.bit_length() - 1)]
    rows_all[:own] = rms_scale(middle.astype(jnp.float32), pre_gain[...]).astype(jnp.bfloat16)
    along = {}
    to_pair = []

    def row_block(zr, dc=0):
        return pl.ds(dc * line + mirror(zr, nz) * own, own)

    def hand_on(zr):
        if zr:
            along[zr].wait_recv()
        for bit in reversed(bits):
            if zr == 0 or bit < (zr & -zr):
                along[zr ^ bit] = links.copy(
                    rows_all.at[row_block(zr)],
                    rows_all.at[row_block(zr ^ bit)],
                    row_sem,
                    ((zr ^ bit) - 1,),
                    links.far(dz=bit),
                )
        for dc in range(1, nc):
            to_pair.append(
                links.copy(
                    rows_all.at[row_block(zr)],
                    rows_all.at[row_block(zr, dc)],
                    row_pair_sem,
                    (zr, dc - 1),
                    links.far(dc=dc),
                )
            )

    hand_on(0)
    each(weights.along_z, 1, far)
    each(weights.spread, 0, far)
    each(weights.relay, 0, near)
    meanwhile = [
        [
            (weights.relay, 0, far),
            (weights.spread, 1, near),
            (weights.relay, 1, near),
            (weights.spread, 1, far),
        ]
    ]
    for zr in sorted(range(1, nz), key=lambda zr: -(zr & -zr)):
        hand_on(zr)
        for item in meanwhile.pop(0) if meanwhile else ():
            each(*item)
    each(weights.along_z, 2, far)
    for items in meanwhile:
        for item in items:
            each(*item)
    each(weights.relay, 1, far)
    each(weights.spread, 2, near)
    each(weights.relay, 2, near)
    for made in to_pair:
        made.wait_recv()
    for j in range(2):
        for zr in range(nz):
            weights.need(j, zr)

    valid = []
    for slot in range(nx):
        at = lax.broadcasted_iota(jnp.int32, (1, weights.wide), 1)
        limit = jnp.where(weights.last(slot), weights.thin, weights.wide)
        valid.append(jnp.where(at < limit, 1.0, 0.0))
    valid = jnp.concatenate(valid, axis=1)

    def mix(b, carry):
        at = span(b, line)
        gate = dot32(rows_all[at, :], held[0])
        up = dot32(rows_all[at, :], held[1])
        hidden[at, :] = jnp.where(valid > 0.0, jax.nn.silu(gate) * up, 0.0).astype(jnp.bfloat16)
        return carry

    lax.fori_loop(0, nc, mix, 0)
    each(weights.spread, 2, far)

    slab = ny * weights.depth
    others = {}
    parts = {}

    def place_of(q):
        return span(flip(links.z, q), slab)

    def project(q):
        weights.need(2, q)
        at = place_of(q)
        value = across(hidden[...], held[2, at, :])
        sums[:, at] = value[:line]
        for dc in range(1, nc):
            other[dc - 1, :, at] = value[dc * line : (dc + 1) * line].astype(jnp.bfloat16)
            others[q, dc] = links.copy(
                other.at[dc - 1, :, at],
                other_land.at[dc - 1, :, at],
                other_sem,
                (q, dc - 1),
                links.far(dc=nc - dc),
            )

    def give(q, level, value):
        if level == len(bits):
            sums[:own, place_of(q)] = value
            return
        at = place_of(q)
        count = value.shape[0] // 2
        half_rows = pl.ds(count, count)
        sums[:count, at] = value[:count]
        sums_send[half_rows, at] = value[count:].astype(jnp.bfloat16)
        parts[q ^ bits[level], level] = links.copy(
            sums_send.at[half_rows, at],
            sums_land.at[half_rows, at],
            sums_sem,
            (q ^ bits[level], level),
            links.far(dz=bits[level]),
        )

    def take(q, level):
        at = place_of(q)
        count = line >> (level + 1)
        parts[q, level].wait_recv()
        land = sums_land[pl.ds(count, count), at].astype(jnp.float32)
        give(q, level + 1, sums[:count, at] + land)

    def settle(q):
        at = place_of(q)
        value = sums[:, at]
        for dc in range(1, nc):
            others[q, dc].wait_recv()
            value = value + other_land[dc - 1, :, at].astype(jnp.float32)
        give(q, 0, value)

    ready = min(2, nz)
    for q in range(ready):
        project(q)
    for q in range(ready):
        settle(q)
    each(weights.relay, 2, far)
    if bits:
        for q in range(ready):
            take(q, 0)
    for q in range(ready, nz):
        project(q)
    for q in range(ready, nz):
        settle(q)
    for q in range(ready, nz):
        take(q, 0)
    for level in range(1, len(bits)):
        for q in range(nz):
            take(q, level)
    total = sums[:own, :]
    out[...] = (middle.astype(jnp.float32) + 0.5 * rms_scale(total, post_gain[...])).astype(
        jnp.bfloat16
    )
    for wait in links.sent:
        wait()
    for d, copy in enumerate(copies, 1):
        pl.when(me + d < n)(copy.wait_send)


def shards(
    n,
    nt,
    residual,
    inputs,
    pole_real,
    pole_imaginary,
    step_log,
    input_real,
    entry_map_quadrature,
    output_real,
    output_imaginary,
    added_log_decay,
    out_weight,
    mix_gain,
    gate_weight,
    up_weight,
    down_weight,
    pre_gain,
    post_gain,
):
    rows, channels = inputs.shape
    columns = out_weight.shape[1]
    groups, states = pole_real.shape
    width = input_real.shape[2]
    flat = groups * states
    step_size = jnp.exp(step_log)[:, None]
    log_size = pole_real * step_size
    angle = pole_imaginary * step_size
    cosine = jnp.cos(angle)
    sine = jnp.sin(angle)
    magnitude = jnp.exp(log_size)
    lift_real = jnp.expm1(log_size) * cosine - 2.0 * jnp.sin(0.5 * angle) ** 2
    lift_imaginary = magnitude * sine
    denominator = pole_real * pole_real + pole_imaginary * pole_imaginary
    ratio_real = (lift_real * pole_real + lift_imaginary * pole_imaginary) / denominator
    ratio_imaginary = (lift_imaginary * pole_real - lift_real * pole_imaginary) / denominator
    lines = jnp.stack(
        (magnitude * cosine, magnitude * sine, ratio_real, ratio_imaginary)
    ).reshape(4, flat)
    entry = jnp.stack((input_real, entry_map_quadrature)).transpose(0, 3, 1, 2)
    read = jnp.stack((output_real, output_imaginary)).transpose(0, 2, 1, 3)
    vmem = pl.BlockSpec(memory_space=pltpu.VMEM)
    nz = math.gcd(n, nt)
    nz = nz & -nz
    ny, nx = n // nz, nt // CORES
    own = rows // nt
    line = nz * own
    depth, units = gate_weight.shape
    piece = -(-units // (LANES * nz)) * LANES
    bf, f32 = jnp.bfloat16, jnp.float32
    return pl.pallas_call(
        functools.partial(layer_kernel, n, nt, nz),
        out_shape=jax.ShapeDtypeStruct((own, columns), bf),
        in_specs=[vmem] * 10 + [pl.BlockSpec(memory_space=pl.ANY)] * 3,
        out_specs=vmem,
        scratch_shapes=[
            pltpu.VMEM((rows, flat), f32),
            pltpu.VMEM((rows, flat), f32),
            pltpu.VMEM((rows, flat), f32),
            pltpu.VMEM((4, CHUNKS, flat), f32),
            pltpu.VMEM((8, flat // 2), f32),
            pltpu.VMEM((n, 8, flat // 2), f32),
            pltpu.VMEM((2, CHUNKS, flat), f32),
            pltpu.VMEM((rows, channels), bf),
            pltpu.VMEM((rows, columns), bf),
            pltpu.VMEM((CORES - 1, nx, own, columns), bf),
            pltpu.VMEM((nx - 1, own, columns), bf),
            pltpu.VMEM((nx - 1, own, columns), bf),
            pltpu.VMEM((3, depth, units), bf),
            pltpu.VMEM((3, n * depth, nx * piece), bf),
            pltpu.VMEM((CORES * line, columns), bf),
            pltpu.VMEM((CORES * line, nx * piece), bf),
            pltpu.VMEM((CORES - 1, line, columns), bf),
            pltpu.VMEM((CORES - 1, line, columns), bf),
            pltpu.VMEM((line, columns), f32),
            pltpu.VMEM((line, columns), bf),
            pltpu.VMEM((line, columns), bf),
            pltpu.SemaphoreType.DMA((n - 1,)),
            pltpu.SemaphoreType.DMA((n - 1,)),
            pltpu.SemaphoreType.DMA((2, 3)),
            pltpu.SemaphoreType.DMA((2, 3, nz - 1)),
            pltpu.SemaphoreType.DMA((2, 3, nz, nx - 1)),
            pltpu.SemaphoreType.DMA((2, 3, nz, ny - 1)),
            pltpu.SemaphoreType.DMA((2, 3, nz, nx - 1, ny - 1)),
            pltpu.SemaphoreType.DMA((2, CORES - 1, nx)),
            pltpu.SemaphoreType.DMA((2, nx - 1)),
            pltpu.SemaphoreType.DMA((2, nz - 1)),
            pltpu.SemaphoreType.DMA((2, nz, CORES - 1)),
            pltpu.SemaphoreType.DMA((2, nz, CORES - 1)),
            pltpu.SemaphoreType.DMA((2, nz, nz.bit_length())),
        ],
        compiler_params=pltpu.CompilerParams(
            collective_id=0, has_side_effects=True, vmem_limit_bytes=60 * 1024 * 1024
        ),
    )(
        inputs,
        added_log_decay,
        lines,
        entry.reshape(2, width, flat),
        read.reshape(2, width, flat),
        residual,
        out_weight,
        mix_gain.reshape(1, columns),
        pre_gain.reshape(1, columns),
        post_gain.reshape(1, columns),
        gate_weight,
        up_weight,
        down_weight,
    )


def solution(mesh):
    return jax.shard_map(
        functools.partial(shards, mesh.shape["sp"], mesh.shape["tp"]),
        mesh=mesh,
        in_specs=(
            P(("sp", "tp"), None),
            P("sp", "tp"),
            P("tp", None),
            P("tp", None),
            P("tp"),
            P("tp", None, None),
            P("tp", None, None),
            P("tp", None, None),
            P("tp", None, None),
            P("sp", "tp"),
            P("tp", None),
            P(),
            P("sp", "tp"),
            P("sp", "tp"),
            P("sp", "tp"),
            P(),
            P(),
        ),
        out_specs=P(("sp", "tp"), None),
        check_vma=False,
    )
```
